768 devices in a mesh: ep: 48 (over z, x), tp: 16 (over y, core).
Axes of the slice: x: 4, y: 8, z: 12, core: 2. Of those that a mesh axis runs over, the one named last changes fastest.
Arguments:
- tokens: bfloat16 [336, 2304], P('ep'), may hold values from -6 to 6
- attn_gain: bfloat16 [2304], replicated, may hold values from 0.099609375 to 1.8984375
- query_weight: bfloat16 [2304, 2048], P(None, 'tp'), may hold values from -0.125 to 0.125
- key_weight: bfloat16 [2304, 2048], P(None, 'tp'), may hold values from -0.125 to 0.125
- value_weight: bfloat16 [2304, 2048], P(None, 'tp'), may hold values from -0.125 to 0.125
- out_weight: bfloat16 [2304, 2048], P(None, 'tp'), may hold values from -0.125 to 0.125
- lambdas: float32 [16], P('tp'), may hold values from 0.3 to 0.8
- head_gain: bfloat16 [128], replicated, may hold values from 0.099609375 to 1.8984375
- cache_keys: bfloat16 [336, 1024, 16, 128], P('ep', None, 'tp'), may hold values from -1500 to 1500
- cache_values: bfloat16 [336, 1024, 16, 128], P('ep', None, 'tp'), may hold values from -6 to 6
- lengths: int32 [336], P('ep'), may hold values from 2 to 1024, as said below
- moe_gain: bfloat16 [2304], replicated, may hold values from 0.099609375 to 1.8984375
- gate_weight: bfloat16 [48, 2304, 1024], P('ep', None, 'tp'), may hold values from -0.125 to 0.125
- up_weight: bfloat16 [48, 2304, 1024], P('ep', None, 'tp'), may hold values from -0.125 to 0.125
- down_weight: bfloat16 [48, 1024, 2304], P('ep', 'tp'), may hold values from -0.1875 to 0.1875
- shared_gate: bfloat16 [2304, 1024], P(None, 'tp'), may hold values from -0.125 to 0.125
- shared_up: bfloat16 [2304, 1024], P(None, 'tp'), may hold values from -0.125 to 0.125
- shared_down: bfloat16 [1024, 2304], P('tp'), may hold values from -0.1875 to 0.1875
- expert_ids: int32 [336, 6], P('ep'), may hold values from 0 to 47, all different within a row; in each aligned block of 7 rows (0 to 6, 7 to 13, ...) at most 2 rows name the same one
- expert_weights: float32 [336, 6], P('ep'), may hold values from 0.2 to 1
Outputs:
- result: bfloat16 [336, 2304], P('ep', 'tp')
The draws below stay inside these ranges and needn't reach their ends.
Inputs may be any that keep to these rules, and one draw needn't show every extreme that they name: `expert_ids`: each row names 6 different experts. Among the rows of one device (aligned blocks of 7 rows) no expert is named by more than 2 rows, a bound that some block reaches. `lengths`: some sequence has 1024 cached positions.
All inputs are finite; a program needn't handle non-finite values.
Results may differ from the reference program's by a relative error of at most 0.02.
Values may be sent and summed in bfloat16 or wider, within the bound.
A program may use at most 32 MiB of HBM per device.

```python
import math
import jax
import jax.numpy as jnp
import numpy as np
from jax import lax

D = 2304
HEADS = 16
HD = 64
VD = 128
EW = 1024
SW = 1024
TOP = 6
SEQ_DEV = 7
CACHE_LEN = 1024
SEQS = 336
EXPERTS = 48
CAP = 2
N_EP = 48
N_TP = 16


def draw_cache_keys(key, part):
    base_draw = jnp.clip(jax.random.normal(key, (SEQS, CACHE_LEN, HEADS, 2 * HD), jnp.float32), -8.0, 8.0) * 1.75
    return base_draw.astype(jnp.bfloat16)


def draw_lengths(key, part):
    key_one, key_two = jax.random.split(jax.random.fold_in(key, 3))
    group_count = SEQS // SEQ_DEV
    group_top = jax.random.randint(key_one, (group_count, 1), CACHE_LEN // 4, CACHE_LEN + 1)
    drawn = jax.random.randint(key_two, (group_count, SEQ_DEV), 2, group_top + 1)
    drawn = drawn.reshape(-1).astype(jnp.int32)
    return drawn.at[0].set(CACHE_LEN)


def steps_of(rng, dims, pieces, least, high):
    def one(axis_at, blocks):
        heights = jax.random.uniform(jax.random.fold_in(jax.random.fold_in(rng, 6), axis_at), (blocks,), jnp.float32, least / len(pieces), high / len(pieces))
        return jnp.repeat(jnp.exp(heights), dims[axis_at] // blocks).reshape((-1,) + (1,) * (len(dims) - axis_at - 1))

    level = one(*pieces[0])
    for cut in pieces[1:]:
        level = level * one(*cut)
    return level


def routed_block(key, own, number, rows, count, top, bound, lean):
    order = jax.random.permutation(key, count)
    heavy_load, usual = shares(count, rows * top, bound, lean, True), shares(count, rows * top, bound, lean, False)
    places = jnp.arange(count)

    def named(tallies, offset_by):
        used = int((tallies > 0).sum())
        fixed = max(1, used // 4)
        moved = fixed + (places - fixed + offset_by * (used - fixed)) % max(1, count - fixed)
        return jnp.zeros((count,), jnp.int32).at[order[jnp.where(places < fixed, places, moved)]].set(jnp.asarray(tallies, jnp.int32))

    tallies = jnp.where(number % 4 == 0, named(heavy_load, number // 4), named(usual, number - number // 4 - 1))
    mixed = jax.random.permutation(jax.random.fold_in(own, 3), count)
    source_of, receiver = mixed[0:count // 2 * 2:2], mixed[1:count // 2 * 2:2]
    margin = jnp.minimum(tallies[source_of] - 1, bound - tallies[receiver]) // 2
    margin = jnp.where((source_of == order[0]) | (receiver == order[0]) | (tallies[receiver] == 0), 0, jnp.maximum(margin, 0))
    moved = jax.random.randint(jax.random.fold_in(own, 4), (count // 2,), 0, 1 << 20) % (margin + 1)
    tallies = tallies.at[source_of].add(-moved).at[receiver].add(moved)
    items = jnp.searchsorted(jnp.cumsum(tallies), jnp.arange(rows * top), side="right").astype(jnp.int32)
    grid = items.reshape(top, rows).T
    grid = grid[jax.random.permutation(jax.random.fold_in(own, 1), rows)]
    offset_by = jax.random.randint(jax.random.fold_in(own, 2), (rows, 1), 0, top)
    return jnp.take_along_axis(grid, (jnp.arange(top)[None, :] + offset_by) % top, axis=1)


def shares(count, total, limit, slope, full):
    portions = [(1 << 20) // math.isqrt(rank ** slope) + 1 for rank in range(1, count + 1)]
    largest = limit if full else min(limit, max(-(-total // count), total * portions[0] // sum(portions)))
    least = 1 if total - largest >= count - 1 else 0
    counts, spare = [largest] + [least] * (count - 1), total - largest - least * (count - 1)
    while spare > 0:
        candidates = [i for i in range(1, count) if counts[i] < largest] or [i for i in range(1, count) if counts[i] < limit]
        pool, remaining = sum([portions[i] for i in candidates]), spare
        for i in candidates:
            extra = min(limit - counts[i], max(1, remaining * portions[i] // pool), spare)
            counts[i] = counts[i] + extra
            spare = spare - extra
    return np.array(counts)


def bell_draw(rng, dims, width, limit, pieces=(), kind=jnp.bfloat16):
    result = width * jax.random.normal(rng, dims, jnp.float32)
    if pieces:
        result = result * steps_of(rng, dims, pieces, -0.22, 0.18)
    return jnp.clip(result, -limit, limit).astype(kind)


def setup_inputs(seed: int = 0) -> dict:
    splits = jax.random.split(jax.random.key(seed), 21)
    tokens = bell_draw(splits[0], (SEQS, D), 1.0, 6.0, ((0, 48),))
    attn_gain = jnp.clip(1.0 + 0.18 * jax.random.normal(splits[1], (D,), jnp.float32), 0.099609375, 1.8984375).astype(jnp.bfloat16)
    query_weight = bell_draw(splits[2], (D, HEADS * 2 * HD), D ** -0.5, 0.125, ((1, 16),))
    key_weight = bell_draw(splits[3], (D, HEADS * 2 * HD), D ** -0.5, 0.125, ((1, 16),))
    value_weight = bell_draw(splits[4], (D, HEADS * VD), D ** -0.5, 0.125, ((1, 16),))
    out_weight = bell_draw(splits[5], (D, HEADS * VD), (HEADS * VD) ** -0.5, 0.125, ((1, 16),))
    lambdas = jnp.clip(0.3 + 0.5 * jax.random.uniform(splits[6], (HEADS,), jnp.float32) ** steps_of(splits[6], (HEADS,), ((0, 16),), -0.2, 0.2), 0.3, 0.8)
    head_gain = jnp.clip(1.0 + 0.18 * jax.random.normal(splits[7], (VD,), jnp.float32), 0.099609375, 1.8984375).astype(jnp.bfloat16)
    cache_keys = draw_cache_keys(jax.random.fold_in(splits[20], 71), 0)
    cache_values = bell_draw(splits[9], (SEQS, CACHE_LEN, HEADS, VD), 1.0, 6.0, ((0, 48), (2, 16)))
    lengths = draw_lengths(jax.random.fold_in(splits[20], 71), 0)
    moe_gain = jnp.clip(1.0 + 0.18 * jax.random.normal(splits[11], (D,), jnp.float32), 0.099609375, 1.8984375).astype(jnp.bfloat16)
    gate_weight = bell_draw(splits[12], (EXPERTS, D, EW), D ** -0.5, 0.125, ((0, 48), (2, 16)))
    up_weight = bell_draw(splits[13], (EXPERTS, D, EW), D ** -0.5, 0.125, ((0, 48), (2, 16)))
    down_weight = bell_draw(splits[14], (EXPERTS, EW, D), EW ** -0.5, 0.1875, ((0, 48), (1, 16)))
    shared_gate = bell_draw(splits[15], (D, SW), D ** -0.5, 0.125, ((1, 16),))
    shared_up = bell_draw(splits[16], (D, SW), D ** -0.5, 0.125, ((1, 16),))
    shared_down = bell_draw(splits[17], (SW, D), SW ** -0.5, 0.1875, ((0, 16),))
    expert_ids_keys = jax.random.split(jax.random.fold_in(splits[18], 1), SEQS // SEQ_DEV)
    expert_ids_turns = jax.random.permutation(jax.random.fold_in(splits[18], 3), SEQS // SEQ_DEV)
    expert_ids = jax.vmap(lambda own, number: routed_block(jax.random.fold_in(splits[18], 2), own, number, SEQ_DEV, EXPERTS, TOP, CAP, 2))(expert_ids_keys, expert_ids_turns).reshape((SEQS, TOP))
    expert_weights = jnp.clip(0.2 + 0.8 * jax.random.uniform(splits[19], (SEQS, TOP), jnp.float32) ** steps_of(splits[19], (SEQS, TOP), ((0, 48),), -0.2, 0.2), 0.2, 1.0)
    return {"tokens": tokens, "attn_gain": attn_gain, "query_weight": query_weight, "key_weight": key_weight, "value_weight": value_weight, "out_weight": out_weight, "lambdas": lambdas, "head_gain": head_gain, "cache_keys": cache_keys, "cache_values": cache_values, "lengths": lengths, "moe_gain": moe_gain, "gate_weight": gate_weight, "up_weight": up_weight, "down_weight": down_weight, "shared_gate": shared_gate, "shared_up": shared_up, "shared_down": shared_down, "expert_ids": expert_ids, "expert_weights": expert_weights}


epsilon = 1e-06

def rms_scale(values, gain):
    wide = values.astype(jnp.float32)
    return wide * lax.rsqrt(lax.optimization_barrier(jnp.mean(wide * wide, axis=-1, keepdims=True)) + epsilon) * gain.astype(jnp.float32)

def rounded(values):
    return lax.optimization_barrier(values.astype(jnp.bfloat16)).astype(jnp.float32)

def attend_group(blocks, lambdas):
    query_rows, key_rows, value_rows, past_keys, past_values, seq_lengths = blocks
    seq_count = query_rows.shape[0]
    head_dim = past_keys.shape[-1] // 2
    score_scale = head_dim ** (-0.5)
    queries = query_rows.astype(jnp.float32).reshape(seq_count, HEADS, 2, head_dim)
    new_keys = key_rows.astype(jnp.float32).reshape(seq_count, HEADS, 2, head_dim)
    new_values = value_rows.astype(jnp.float32).reshape(seq_count, HEADS, 2 * head_dim)
    cache_rows = past_keys.astype(jnp.float32).reshape(seq_count, CACHE_LEN, HEADS, 2, head_dim)
    scores = jnp.einsum('shmd,sjhmd->shmj', queries, cache_rows) * score_scale
    own_score = lax.optimization_barrier(jnp.sum(queries * new_keys, axis=-1)) * score_scale
    live_mask = (jnp.arange(CACHE_LEN, dtype=jnp.int32)[None, :] < seq_lengths[:, None])[:, None, None, :]
    peak_score = jnp.maximum(lax.optimization_barrier(jnp.max(jnp.where(live_mask, scores, -jnp.inf), axis=-1)), own_score)
    exp_terms = jnp.where(live_mask, jnp.exp(scores - peak_score[..., None]), 0.0)
    own_term = jnp.exp(own_score - peak_score)
    denom_sum = lax.optimization_barrier(jnp.sum(exp_terms, axis=-1)) + own_term
    map_probs = exp_terms / denom_sum[..., None]
    own_prob = own_term / denom_sum
    lambda_row = lambdas[None, :]
    mixture = rounded(map_probs[:, :, 0] - lambda_row[..., None] * map_probs[:, :, 1])
    own_mixture = rounded(own_prob[:, :, 0] - lambda_row * own_prob[:, :, 1])
    head_out = jnp.einsum('shj,sjhv->shv', mixture, past_values.astype(jnp.float32))
    return head_out + own_mixture[..., None] * new_values

def reference(tokens, attn_gain, query_weight, key_weight, value_weight, out_weight, lambdas, head_gain, cache_keys, cache_values, lengths, moe_gain, gate_weight, up_weight, down_weight, shared_gate, shared_up, shared_down, expert_ids, expert_weights):
    normed = rms_scale(tokens, attn_gain).astype(jnp.bfloat16)
    query_rows = jnp.dot(normed, query_weight, preferred_element_type=jnp.float32).astype(jnp.bfloat16)
    key_new = jnp.dot(normed, key_weight, preferred_element_type=jnp.float32).astype(jnp.bfloat16)
    value_new = jnp.dot(normed, value_weight, preferred_element_type=jnp.float32).astype(jnp.bfloat16)

    def grouped(array):
        return array.reshape((N_EP, SEQ_DEV) + array.shape[1:])
    head_out = lax.map(lambda blocks: attend_group(blocks, lambdas), (grouped(query_rows), grouped(key_new), grouped(value_new), grouped(cache_keys), grouped(cache_values), grouped(lengths)))
    head_out = head_out.reshape(SEQS, HEADS, VD)
    head_normed = rms_scale(head_out, head_gain).astype(jnp.bfloat16)
    group_cols = HEADS * VD // N_TP
    head_groups = head_normed.reshape(SEQS, N_TP, group_cols).astype(jnp.float32)
    out_groups = out_weight.reshape(D, N_TP, group_cols).astype(jnp.float32)
    attn_part = rounded(jnp.einsum('snc,dnc->nsd', head_groups, out_groups))
    mixed_rows = (tokens.astype(jnp.float32) + lax.optimization_barrier(jnp.sum(attn_part, axis=0))).astype(jnp.bfloat16)
    moe_normed = rms_scale(mixed_rows, moe_gain).astype(jnp.bfloat16)
    shared_gate_out = jnp.dot(moe_normed, shared_gate, preferred_element_type=jnp.float32)
    shared_up_out = jnp.dot(moe_normed, shared_up, preferred_element_type=jnp.float32)
    shared_hidden = (jax.nn.silu(shared_gate_out) * shared_up_out).astype(jnp.bfloat16)
    shared_cols = SW // N_TP
    shared_part = rounded(jnp.einsum('snc,ncd->nsd', shared_hidden.reshape(SEQS, N_TP, shared_cols).astype(jnp.float32), shared_down.reshape(N_TP, shared_cols, D).astype(jnp.float32)))
    shared_out = lax.optimization_barrier(jnp.sum(shared_part, axis=0))
    slot_ids = expert_ids.reshape(N_EP, SEQ_DEV * TOP).astype(jnp.int32)
    expert_hits = (slot_ids[..., None] == jnp.arange(EXPERTS, dtype=jnp.int32)[None, None, :]).astype(jnp.int32)
    earlier = jnp.cumsum(expert_hits, axis=1).astype(jnp.int32) - expert_hits
    slot_rank = lax.optimization_barrier(jnp.sum(earlier * expert_hits, axis=-1)).astype(jnp.int32)
    slot_row = (jnp.arange(N_EP, dtype=jnp.int32)[:, None] * CAP + slot_rank).reshape(-1)
    slot_token = (jnp.arange(SEQS * TOP, dtype=jnp.int32) // TOP).astype(jnp.int32)
    flat_ids = slot_ids.reshape(-1)
    expert_rows = jnp.zeros((EXPERTS, N_EP * CAP, D), jnp.bfloat16)
    expert_rows = expert_rows.at[flat_ids, slot_row].set(moe_normed[slot_token])
    expert_cols = EW // N_TP

    def run_expert(blocks):
        row_block, gate_block, up_block, down_block = blocks
        gate_out = jnp.dot(row_block, gate_block, preferred_element_type=jnp.float32)
        up_out = jnp.dot(row_block, up_block, preferred_element_type=jnp.float32)
        expert_hidden = (jax.nn.silu(gate_out) * up_out).astype(jnp.bfloat16)
        partials = jnp.einsum('rnc,ncd->nrd', expert_hidden.reshape(N_EP * CAP, N_TP, expert_cols).astype(jnp.float32), down_block.reshape(N_TP, expert_cols, D).astype(jnp.float32))
        return lax.optimization_barrier(jnp.sum(rounded(partials), axis=0)).astype(jnp.bfloat16)
    expert_out = lax.map(run_expert, (expert_rows, gate_weight, up_weight, down_weight))
    slot_values = expert_out[flat_ids, slot_row].astype(jnp.float32).reshape(SEQS, TOP, D)
    routed = lax.optimization_barrier(jnp.sum(expert_weights[:, :, None] * slot_values, axis=1))
    return (mixed_rows.astype(jnp.float32) + routed + shared_out).astype(jnp.bfloat16)
```

```python
import functools

import jax
import jax.numpy as jnp
from jax import lax
from jax.experimental import pallas as pl
from jax.experimental.pallas import tpu as pltpu
from jax.sharding import PartitionSpec as P

EPS = 1e-06
NX = 4
MESH = pl.DeviceIdType.MESH
NT = (((1,), (1,)), ((), ()))
bf16, f32, i32 = jnp.bfloat16, jnp.float32, jnp.int32
SLOT = 144
LANES = 256


def wrap(v, n):
    return jnp.where(v < 0, v + n, v)


def mm(a, b):
    return jnp.dot(a, b, preferred_element_type=f32)


def mm_nt(a, b):
    return lax.dot_general(a, b, NT, preferred_element_type=f32)


def kernel(
    n_ep, n_tp,
    tok, again, wq, wk, wv, ow, lam, hgain, ck, cv, lens, mgain, gwt, uwt, dw, sgt, sut, sd, ids, ew,
    out,
    tok_v, wqkv, k_v, v_v, ow_v, wt, dcat, lam_s, lens_s, again_v, hgain_v, mgain_v, ids_v, ew_v,
    x_s, tokblk, idp, ewp, dnt, gainb,
    send1, recv1, send2, recv2, xt, pt, sib, q5, recv5, send6, recv6,
    lsem, ssem, rsem, s3, r3, f3s, f3r, s5a, r5a, s5, r5,
):
    n_z, n_y = n_ep // NX, n_tp // 2
    seqs, width = tok.shape
    cache = ck.shape[1]
    me_ep, me_tp = lax.axis_index("ep"), lax.axis_index("tp")
    z, x = me_ep // NX, lax.rem(me_ep, NX)
    y, c = me_tp // 2, lax.rem(me_tp, 2)

    def ep_at(slot):
        dz, dx = slot // NX, slot % NX
        return lax.rem(z + dz, n_z) * NX + lax.rem(x + dx, NX)

    def ep_back(slot):
        dz, dx = slot // NX, slot % NX
        return lax.rem(z + n_z - dz, n_z) * NX + lax.rem(x + NX - dx, NX)

    bar = pltpu.get_barrier_semaphore()
    for r in range(1, n_tp):
        pl.semaphore_signal(bar, inc=1, device_id={"tp": lax.rem(me_tp + r, n_tp)}, device_id_type=MESH)

    def greet(i, carry):
        pl.semaphore_signal(bar, inc=1, device_id={"ep": ep_at(i)}, device_id_type=MESH)
        return carry

    loads = []

    def load(src, dst):
        cp = pltpu.make_async_copy(src, dst, lsem.at[len(loads)])
        cp.start()
        loads.append(cp)
        return cp

    c_tok = [load(tok, tok_v), load(again, again_v)]
    c_qkv = [load(w, wqkv.at[:, pl.ds(128 * i, 128)]) for i, w in enumerate((wq, wk, wv))]
    c_len = [load(lens, lens_s), load(lam, lam_s), load(hgain, hgain_v)]
    c_k = [load(ck.at[s], k_v.at[s // 2, :, pl.ds(128 * (s % 2), 128)]) for s in range(seqs)]
    c_v = [load(cv.at[s], v_v.at[s // 2, :, pl.ds(128 * (s % 2), 128)]) for s in range(seqs)]
    c_ow = [load(ow.at[pl.ds(SLOT * t, SLOT)], ow_v.at[t, pl.ds(0, SLOT)]) for t in range(n_tp)]
    lax.fori_loop(1, n_ep, greet, 0)
    c_ids = [load(ids, ids_v), load(ew, ew_v), load(mgain, mgain_v)]
    c_wt = [load(w, wt.at[pl.ds(64 * i, 64)]) for i, w in enumerate((gwt, uwt, sgt, sut))]
    c_dn = [load(w, dcat.at[pl.ds(64 * i, 64)]) for i, w in enumerate((dw, sd))]

    def done(cps):
        for cp in cps:
            cp.wait()

    x_s[...] = jnp.zeros_like(x_s)
    if seqs % 2:
        k_v[seqs // 2, :, pl.ds(128, 128)] = jnp.zeros((cache, 128), bf16)
        v_v[seqs // 2, :, pl.ds(128, 128)] = jnp.zeros((cache, 128), bf16)
    done(c_tok)
    x_s[0:seqs, :] = tok_v[...].astype(f32)
    xv = x_s[...]
    gain = again_v[...].astype(f32).reshape(1, width)
    normed = (xv * lax.rsqrt(jnp.mean(xv * xv, axis=-1, keepdims=True) + EPS) * gain).astype(bf16)
    done(c_qkv)
    qkv = mm(normed, wqkv[...]).astype(bf16).astype(f32)
    q, kn, vn = qkv[:, 0:128], qkv[:, 128:256], qkv[:, 256:384]
    lane = lax.broadcasted_iota(i32, (8, 128), 1)
    first = lane < 64
    qk = q * kn
    scale = 0.125
    own = jnp.concatenate(
        [jnp.sum(jnp.where(first, qk, 0.0), axis=-1, keepdims=True),
         jnp.sum(jnp.where(first, 0.0, qk), axis=-1, keepdims=True)], axis=0) * scale
    q2 = jnp.concatenate([jnp.where(first, q, 0.0), jnp.where(first, 0.0, q)], axis=0)
    row16 = lax.broadcasted_iota(i32, (16, 128), 0)
    row16 = jnp.where(row16 >= 8, row16 - 8, row16)
    scores = jnp.zeros((16, cache), f32)
    done(c_len)
    for p in range((seqs + 1) // 2):
        done(c_k[2 * p : 2 * p + 2])
        qa = jnp.where(row16 == 2 * p, q2, 0.0)
        qb = jnp.where(row16 == 2 * p + 1, q2, 0.0)
        scores += mm_nt(jnp.concatenate([qa, qb], axis=1).astype(bf16), k_v[p])
    scores = scores * scale
    rcol = lax.broadcasted_iota(i32, (16, 1), 0)
    rcol = jnp.where(rcol >= 8, rcol - 8, rcol)
    lcol = jnp.zeros((16, 1), i32)
    for s in range(seqs):
        lcol = jnp.where(rcol == s, lens_s[s], lcol)
    live = lax.broadcasted_iota(i32, (16, cache), 1) < lcol
    peak = jnp.maximum(jnp.max(jnp.where(live, scores, -jnp.inf), axis=-1, keepdims=True), own)
    terms = jnp.where(live, jnp.exp(scores - peak), 0.0)
    own_term = jnp.exp(own - peak)
    inv = 1.0 / (jnp.sum(terms, axis=-1, keepdims=True) + own_term)
    probs, own_prob = terms * inv, own_term * inv
    lm = lam_s[0]
    mix = (probs[0:8] - lm * probs[8:16]).astype(bf16).astype(f32)
    own_mix = (own_prob[0:8] - lm * own_prob[8:16]).astype(bf16).astype(f32)
    rowc = lax.broadcasted_iota(i32, (8, cache), 0)
    both = jnp.zeros((8, 256), f32)
    for p in range((seqs + 1) // 2):
        done(c_v[2 * p : 2 * p + 2])
        both += mm(jnp.where(rowc // 2 == p, mix, 0.0).astype(bf16), v_v[p])
    row8 = lax.broadcasted_iota(i32, (8, 128), 0)
    head = jnp.where(row8 % 2 == 0, both[:, 0:128], both[:, 128:256]) + own_mix * vn
    hg = hgain_v[...].astype(f32).reshape(1, 128)
    head_n = (head * lax.rsqrt(jnp.mean(head * head, axis=-1, keepdims=True) + EPS) * hg).astype(bf16)
    done(c_ow)
    part = mm_nt(head_n, ow_v[...].reshape(n_tp * LANES, 128)).astype(bf16)
    for t in range(n_tp):
        send1[t] = part[:, LANES * t : LANES * (t + 1)]

    pl.semaphore_wait(bar, n_tp - 1 + n_ep - 1)
    for r in sorted(range(1, n_tp), key=lambda r: -min(r, n_tp - r)):
        to = lax.rem(me_tp + r, n_tp)
        pltpu.make_async_remote_copy(
            src_ref=send1.at[to], dst_ref=recv1.at[r - 1], send_sem=ssem.at[0], recv_sem=rsem.at[0],
            device_id={"tp": to}, device_id_type=MESH).start()

    for t in range(n_tp):
        tokblk[t, :, pl.ds(0, SLOT)] = xv[:, SLOT * t : SLOT * (t + 1)]
    done(c_ids)
    idp[...] = jnp.full_like(idp, -1)
    ewp[...] = jnp.zeros_like(ewp)
    idp[0:seqs, 0 : ids.shape[1]] = ids_v[...]
    ewp[0:seqs, 0 : ids.shape[1]] = ew_v[...]
    idv, ewv = idp[...], ewp[...]
    rid = wrap((idv >> 2) - z, n_z) * NX + wrap((idv & 3) - x, NX)
    rid = jnp.where(idv < 0, -1, rid)
    slot_l, rank_l = lane >> 1, lane & 1
    hit, wsum = jnp.zeros((8, 128), f32), jnp.zeros((8, 128), f32)
    for k in range(ids.shape[1]):
        m = rid[:, k : k + 1] == slot_l
        hit = jnp.where(m, 1.0, hit)
        wsum = jnp.where(m, ewv[:, k : k + 1], wsum)
    rank = jnp.zeros((8, 128), f32)
    for s in range(seqs):
        rank += jnp.where(row8 > s, hit[s : s + 1, :], 0.0)
    place = jnp.where(rank == rank_l.astype(f32), hit, 0.0)
    comb = place * wsum
    comb_hi = comb.astype(bf16)
    comb_lo = (comb - comb_hi.astype(f32)).astype(bf16)
    comb2 = jnp.concatenate([comb_hi.astype(f32), comb_lo.astype(f32)], axis=0).astype(bf16)
    place_t = jnp.concatenate([place, jnp.zeros((120, 128), f32)], axis=0).T.astype(bf16)
    done(c_dn)
    for i in range(width // 128):
        cols = pl.ds(128 * i, 128)
        dnt[cols, :] = dcat[:, cols].astype(f32).T.astype(bf16)
    mg = mgain_v[...].astype(f32).reshape(1, width)
    for i in range(width // 128):
        gainb[pl.ds(128 * i, 128), :] = jnp.broadcast_to(mg[:, 128 * i : 128 * (i + 1)], (128, 128)).T

    own_part = send1[me_tp].astype(f32)
    own_tok = tokblk[me_tp]
    pltpu.make_async_copy(recv1, recv1, rsem.at[0]).wait()
    attn = own_part + jnp.sum(recv1[...].astype(f32), axis=0)
    lane2 = lax.broadcasted_iota(i32, (8, LANES), 1)
    mixed = jnp.where(lane2 < SLOT, own_tok + attn, 0.0).astype(bf16)
    mixed_f = mixed.astype(f32)

    mixed_p = jnp.concatenate([mixed_f, jnp.zeros((120, LANES), f32)], axis=0).astype(bf16)
    rows = mm(place_t, mixed_p)[0 : 2 * n_ep].astype(bf16)
    send2[...] = rows.reshape(n_ep, 2, LANES)

    def give(i, carry):
        slot = n_ep - i
        pltpu.make_async_remote_copy(
            src_ref=send2.at[slot], dst_ref=recv2.at[slot], send_sem=ssem.at[1], recv_sem=rsem.at[1],
            device_id={"ep": ep_at(slot)}, device_id_type=MESH).start()
        return carry

    lax.fori_loop(1, n_ep, give, 0)
    recv2[0] = send2[0]
    done(c_wt)
    pltpu.make_async_copy(recv2.at[pl.ds(1, n_ep - 1)], recv2.at[pl.ds(1, n_ep - 1)], rsem.at[1]).wait()
    got = recv2[...].reshape(2 * n_ep, LANES).astype(f32)
    parts = [got, mixed_f]
    if 128 - 2 * n_ep - 8 > 0:
        parts.append(jnp.zeros((128 - 2 * n_ep - 8, LANES), f32))
    rows_t = jnp.concatenate(parts, axis=0).T
    xt[me_tp] = rows_t[0:SLOT].astype(bf16)

    def gather_copy(dy):
        return pltpu.make_async_remote_copy(
            src_ref=xt.at[me_tp], dst_ref=xt.at[me_tp], send_sem=s3.at[dy], recv_sem=r3.at[dy],
            device_id={"tp": lax.rem(y + dy, n_y) * 2 + c}, device_id_type=MESH)

    def hand_copy(dy):
        t = lax.rem(y + n_y - dy, n_y) * 2 + c
        return pltpu.make_async_remote_copy(
            src_ref=xt.at[t], dst_ref=xt.at[t], send_sem=f3s.at[dy], recv_sem=f3r.at[dy],
            device_id={"tp": y * 2 + 1 - c}, device_id_type=MESH)

    far = sorted(range(1, n_y), key=lambda d: -min(d, n_y - d))
    for dy in far:
        gather_copy(dy).start()
    hand_copy(0).start()
    for dy in reversed(far):
        gather_copy(dy).wait_recv()
        hand_copy(dy).start()
    for dy in range(n_y):
        hand_copy(dy).wait_recv()

    xa = xt[...].reshape(width, 128).astype(f32)
    inv_rms = lax.rsqrt(jnp.sum(xa * xa, axis=0, keepdims=True) * (1.0 / width) + EPS)
    xn = (xa * inv_rms * gainb[...]).astype(bf16)
    hid = mm(wt[...], xn)
    ge, ue, gs, us = hid[0:64], hid[64:128], hid[128:192], hid[192:256]
    lane64 = lax.broadcasted_iota(i32, (64, 128), 1)
    routed_l = lane64 < 2 * n_ep
    he = jnp.where(routed_l, ge / (1.0 + jnp.exp(-ge)) * ue, 0.0)
    hs = jnp.where(routed_l, 0.0, gs / (1.0 + jnp.exp(-gs)) * us)
    hcat = jnp.concatenate([he, hs], axis=0).astype(bf16)

    def sib_copy(v):
        t = v * 2 + 1 - c
        return pltpu.make_async_remote_copy(
            src_ref=pt.at[t], dst_ref=sib.at[v], send_sem=s5a.at[v], recv_sem=r5a.at[v],
            device_id={"tp": y * 2 + 1 - c}, device_id_type=MESH)

    def sum_copy(dy):
        v = lax.rem(y + dy, n_y)
        return pltpu.make_async_remote_copy(
            src_ref=q5.at[v], dst_ref=recv5.at[dy], send_sem=s5.at[dy], recv_sem=r5.at[dy],
            device_id={"tp": v * 2 + c}, device_id_type=MESH)

    pt[...] = mm(dnt[...], hcat).astype(bf16).reshape(n_tp, SLOT, 128)
    order = far + [0]
    for dy in order:
        sib_copy(lax.rem(y + dy, n_y)).start()
    for dy in order:
        v = lax.rem(y + dy, n_y)
        sib_copy(v).wait_recv()
        pair = pt[v * 2 + c].astype(f32) + sib[v].astype(f32)
        if dy:
            q5[v] = pair.astype(bf16)
            sum_copy(dy).start()
        else:
            total = pair
    for dy in reversed(far):
        sum_copy(dy).wait_recv()
        total += recv5[dy].astype(f32)
    back = jnp.concatenate([total, jnp.zeros((LANES - SLOT, 128), f32)], axis=0).T
    shared = back[2 * n_ep : 2 * n_ep + 8]
    send6[...] = back[0 : 2 * n_ep].astype(bf16).reshape(n_ep, 2, LANES)

    def give_back(i, carry):
        slot = n_ep - i
        pltpu.make_async_remote_copy(
            src_ref=send6.at[slot], dst_ref=recv6.at[slot], send_sem=ssem.at[2], recv_sem=rsem.at[2],
            device_id={"ep": ep_back(slot)}, device_id_type=MESH).start()
        return carry

    lax.fori_loop(1, n_ep, give_back, 0)
    recv6[0] = send6[0]
    pltpu.make_async_copy(recv1, recv1, ssem.at[0]).wait()
    pltpu.make_async_copy(recv2.at[pl.ds(1, n_ep - 1)], recv2.at[pl.ds(1, n_ep - 1)], ssem.at[1]).wait()
    for dy in range(n_y):
        hand_copy(dy).wait_send()
        sib_copy(dy).wait_send()
        if dy:
            gather_copy(dy).wait_send()
            sum_copy(dy).wait_send()
    pltpu.make_async_copy(recv6.at[pl.ds(1, n_ep - 1)], recv6.at[pl.ds(1, n_ep - 1)], rsem.at[2]).wait()
    vals = recv6[...].reshape(2 * n_ep, LANES)
    two = mm(comb2[:, 0 : 2 * n_ep], vals)
    res = mixed_f + (two[0:8] + two[8:16]) + shared
    out[...] = res[0:seqs, 0:SLOT].astype(bf16)
    pltpu.make_async_copy(recv6.at[pl.ds(1, n_ep - 1)], recv6.at[pl.ds(1, n_ep - 1)], ssem.at[2]).wait()


def solution(mesh):
    n_ep, n_tp = mesh.shape["ep"], mesh.shape["tp"]
    n_y = n_tp // 2

    def step(tokens, attn_gain, wq, wk, wv, ow, lambdas, head_gain, ck, cv, lengths, moe_gain,
             gw, uw, dw, sg, su, sd, ids, ew):
        seqs, width = tokens.shape
        cache = ck.shape[1]
        pairs = (seqs + 1) // 2
        V, DMA = pltpu.VMEM, pltpu.SemaphoreType.DMA
        scratch = [
            V((seqs, width), bf16), V((width, 384), bf16), V((pairs, cache, 256), bf16), V((pairs, cache, 256), bf16),
            V((n_tp, LANES, 128), bf16), V((256, width), bf16), V((128, width), bf16),
            pltpu.SMEM((1,), f32), pltpu.SMEM((seqs,), i32), V((width,), bf16), V((128,), bf16), V((width,), bf16),
            V(ids.shape, i32), V(ew.shape, f32),
            V((8, width), f32), V((n_tp, 8, LANES), f32), V((8, 128), i32), V((8, 128), f32),
            V((width, 128), bf16), V((width, 128), f32),
            V((n_tp, 8, LANES), bf16), V((n_tp - 1, 8, LANES), bf16),
            V((n_ep, 2, LANES), bf16), V((n_ep, 2, LANES), bf16),
            V((n_tp, SLOT, 128), bf16), V((n_tp, SLOT, 128), bf16), V((n_y, SLOT, 128), bf16),
            V((n_y, SLOT, 128), bf16), V((n_y, SLOT, 128), bf16),
            V((n_ep, 2, LANES), bf16), V((n_ep, 2, LANES), bf16),
            DMA((64,)), DMA((3,)), DMA((3,)),
            DMA((n_y,)), DMA((n_y,)), DMA((n_y,)), DMA((n_y,)),
            DMA((n_y,)), DMA((n_y,)), DMA((n_y,)), DMA((n_y,)),
        ]
        return pl.pallas_call(
            functools.partial(kernel, n_ep, n_tp),
            out_shape=jax.ShapeDtypeStruct((seqs, width // n_tp), bf16),
            in_specs=[pl.BlockSpec(memory_space=pl.ANY)] * 20,
            out_specs=pl.BlockSpec(memory_space=pltpu.VMEM),
            scratch_shapes=scratch,
            compiler_params=pltpu.CompilerParams(collective_id=0, has_side_effects=True),
            name="decode_step",
        )(tokens, attn_gain, wq, wk, wv, ow, lambdas, head_gain,
          ck.reshape(seqs, cache, 128), cv.reshape(seqs, cache, 128), lengths, moe_gain,
          gw[0].T, uw[0].T, dw[0], sg.T, su.T, sd, ids, ew)

    in_specs = (
        P("ep", None), P(), P(None, "tp"), P(None, "tp"), P(None, "tp"), P(None, "tp"), P("tp"), P(),
        P("ep", None, "tp", None), P("ep", None, "tp", None), P("ep"), P(),
        P("ep", None, "tp"), P("ep", None, "tp"), P("ep", "tp", None),
        P(None, "tp"), P(None, "tp"), P("tp", None), P("ep", None), P("ep", None),
    )
    return jax.shard_map(step, mesh=mesh, in_specs=in_specs, out_specs=P("ep", "tp"), check_vma=False)
```

```python
import functools

import jax
import jax.numpy as jnp
from jax import lax
from jax.experimental import pallas as pl
from jax.experimental.pallas import tpu as pltpu
from jax.sharding import PartitionSpec as P

EPS = 1e-06
NX = 4
MESH = pl.DeviceIdType.MESH
NT = (((1,), (1,)), ((), ()))
bf16, f32, i32 = jnp.bfloat16, jnp.float32, jnp.int32
SLOT = 144
LANES = 256
REST = SLOT - 128
PAIR = 384


def wrap(v, n):
    return jnp.where(v < 0, v + n, v)


def mm(a, b):
    return jnp.dot(a, b, preferred_element_type=f32)


def mm_nt(a, b):
    return lax.dot_general(a, b, NT, preferred_element_type=f32)


def kernel(
    n_ep, n_tp,
    tok, again, wq, wk, wv, ow, lam, hgain, ck, cv, lens, mgain, gwt, uwt, dw, sgt, sut, sd, ids, ew,
    out,
    tok_v, wqkv, k_v, v_v, ow_v, wt, dcat, lam_s, lens_s, again_v, hgain_v, mgain_v, ids_v, ew_v,
    x_s, tokblk, idp, ewp, dnt, dsib, gainb,
    send1, recv1, send2, recv2, xt, q5, recv5, send6, recv6,
    lsem, ssem, rsem, s3, r3, f3s, f3r, s5, r5, wsem,
):
    n_z, n_y = n_ep // NX, n_tp // 2
    seqs, width = tok.shape
    cache = ck.shape[1]
    me_ep, me_tp = lax.axis_index("ep"), lax.axis_index("tp")
    z, x = me_ep // NX, lax.rem(me_ep, NX)
    y, c = me_tp // 2, lax.rem(me_tp, 2)

    half = n_tp // 2
    pair = lax.rem(me_tp, half)
    other = lax.rem(me_tp + half, n_tp)
    sibling = {"tp": y * 2 + 1 - c}
    z_at = [wrap(z + d - n_z, n_z) * NX for d in range(n_z)]
    x_at = [wrap(x + d - NX, NX) for d in range(NX)]

    def hops(slot):
        dz, dx = slot // NX, slot % NX
        return min(dz, n_z - dz) + min(dx, NX - dx)

    slots = sorted(range(1, n_ep), key=lambda s: -hops(s))

    def ep_at(slot):
        return z_at[slot // NX] + x_at[slot % NX]

    def ep_back(slot):
        return z_at[-(slot // NX) % n_z] + x_at[-(slot % NX) % NX]

    bar = pltpu.get_barrier_semaphore()
    loads = []

    def load(src, dst):
        cp = pltpu.make_async_copy(src, dst, lsem.at[len(loads)])
        cp.start()
        loads.append(cp)
        return cp

    c_tok = [load(tok, tok_v), load(again, again_v)]
    c_qkv = [load(w, wqkv.at[:, pl.ds(128 * i, 128)]) for i, w in enumerate((wq, wk, wv))]
    for r in range(1, n_tp):
        pl.semaphore_signal(bar, inc=1, device_id={"tp": lax.rem(me_tp + r, n_tp)}, device_id_type=MESH)
    c_len = [load(lens, lens_s), load(lam, lam_s), load(hgain, hgain_v)]
    c_k = [load(ck.at[s], k_v.at[s // 2, :, pl.ds(128 * (s % 2), 128)]) for s in range(seqs)]
    c_v = [load(cv.at[s], v_v.at[s // 2, :, pl.ds(128 * (s % 2), 128)]) for s in range(seqs)]
    c_ow = []
    for t in range(n_tp):
        hi = t // half
        c_ow.append(load(ow.at[pl.ds(SLOT * t, 128)], ow_v.at[t % half, pl.ds(128 * hi, 128)]))
        c_ow.append(load(ow.at[pl.ds(SLOT * t + 128, REST)], ow_v.at[t % half, pl.ds(256 + REST * hi, REST)]))
    for slot in slots:
        pl.semaphore_signal(bar, inc=1, device_id={"ep": ep_at(slot)}, device_id_type=MESH)
    c_ids = [load(ids, ids_v), load(ew, ew_v), load(mgain, mgain_v)]
    c_wt = [load(w, wt.at[pl.ds(64 * i, 64)]) for i, w in enumerate((gwt, uwt, sgt, sut))]
    c_dn = [load(w, dcat.at[pl.ds(64 * i, 64)]) for i, w in enumerate((dw, sd))]

    def done(cps):
        for cp in cps:
            cp.wait()

    x_s[...] = jnp.zeros_like(x_s)
    if seqs % 2:
        k_v[seqs // 2, :, pl.ds(128, 128)] = jnp.zeros((cache, 128), bf16)
        v_v[seqs // 2, :, pl.ds(128, 128)] = jnp.zeros((cache, 128), bf16)
    done(c_tok)
    x_s[0:seqs, :] = tok_v[...].astype(f32)
    xv = x_s[...]
    gain = again_v[...].astype(f32).reshape(1, width)
    normed = (xv * lax.rsqrt(jnp.mean(xv * xv, axis=-1, keepdims=True) + EPS) * gain).astype(bf16)
    done(c_qkv)
    qkv = mm(normed, wqkv[...]).astype(bf16).astype(f32)
    q, kn, vn = qkv[:, 0:128], qkv[:, 128:256], qkv[:, 256:384]
    lane = lax.broadcasted_iota(i32, (8, 128), 1)
    first = lane < 64
    qk = q * kn
    scale = 0.125
    own = jnp.concatenate(
        [jnp.sum(jnp.where(first, qk, 0.0), axis=-1, keepdims=True),
         jnp.sum(jnp.where(first, 0.0, qk), axis=-1, keepdims=True)], axis=0) * scale
    q2 = jnp.concatenate([jnp.where(first, q, 0.0), jnp.where(first, 0.0, q)], axis=0)
    row16 = lax.broadcasted_iota(i32, (16, 128), 0)
    row16 = jnp.where(row16 >= 8, row16 - 8, row16)
    scores = jnp.zeros((16, cache), f32)
    done(c_len)
    for p in range((seqs + 1) // 2):
        done(c_k[2 * p : 2 * p + 2])
        qa = jnp.where(row16 == 2 * p, q2, 0.0)
        qb = jnp.where(row16 == 2 * p + 1, q2, 0.0)
        scores += mm_nt(jnp.concatenate([qa, qb], axis=1).astype(bf16), k_v[p])
    scores = scores * scale
    rcol = lax.broadcasted_iota(i32, (16, 1), 0)
    rcol = jnp.where(rcol >= 8, rcol - 8, rcol)
    lcol = jnp.zeros((16, 1), i32)
    for s in range(seqs):
        lcol = jnp.where(rcol == s, lens_s[s], lcol)
    live = lax.broadcasted_iota(i32, (16, cache), 1) < lcol
    peak = jnp.maximum(jnp.max(jnp.where(live, scores, -jnp.inf), axis=-1, keepdims=True), own)
    terms = jnp.where(live, jnp.exp(scores - peak), 0.0)
    own_term = jnp.exp(own - peak)
    inv = 1.0 / (jnp.sum(terms, axis=-1, keepdims=True) + own_term)
    probs, own_prob = terms * inv, own_term * inv
    lm = lam_s[0]
    mix = (probs[0:8] - lm * probs[8:16]).astype(bf16).astype(f32)
    own_mix = (own_prob[0:8] - lm * own_prob[8:16]).astype(bf16).astype(f32)
    rowc = lax.broadcasted_iota(i32, (8, cache), 0)
    both = jnp.zeros((8, 256), f32)
    for p in range((seqs + 1) // 2):
        done(c_v[2 * p : 2 * p + 2])
        both += mm(jnp.where(rowc // 2 == p, mix, 0.0).astype(bf16), v_v[p])
    row8 = lax.broadcasted_iota(i32, (8, 128), 0)
    head = jnp.where(row8 % 2 == 0, both[:, 0:128], both[:, 128:256]) + own_mix * vn
    hg = hgain_v[...].astype(f32).reshape(1, 128)
    head_n = (head * lax.rsqrt(jnp.mean(head * head, axis=-1, keepdims=True) + EPS) * hg).astype(bf16)
    done(c_ow)
    part = mm_nt(head_n, ow_v[...].reshape(half * PAIR, 128)).astype(bf16)
    for p in range(half):
        send1[p] = part[:, PAIR * p : PAIR * (p + 1)]

    pl.semaphore_wait(bar, n_tp - 1 + n_ep - 1)
    for r in sorted(range(1, n_tp), key=lambda r: -min(r, n_tp - r)):
        to = lax.rem(me_tp + r, n_tp)
        pltpu.make_async_remote_copy(
            src_ref=send1.at[lax.rem(to, half)], dst_ref=recv1.at[r - 1], send_sem=ssem.at[0], recv_sem=rsem.at[0],
            device_id={"tp": to}, device_id_type=MESH).start()

    for t in range(n_tp):
        hi = t // half
        tokblk[t % half, :, pl.ds(128 * hi, 128)] = xv[:, SLOT * t : SLOT * t + 128]
        tokblk[t % half, :, pl.ds(256 + REST * hi, REST)] = xv[:, SLOT * t + 128 : SLOT * (t + 1)]
    done(c_ids)
    idp[...] = jnp.full_like(idp, -1)
    ewp[...] = jnp.zeros_like(ewp)
    idp[0:seqs, 0 : ids.shape[1]] = ids_v[...]
    ewp[0:seqs, 0 : ids.shape[1]] = ew_v[...]
    idv, ewv = idp[...], ewp[...]
    rid = wrap((idv >> 2) - z, n_z) * NX + wrap((idv & 3) - x, NX)
    rid = jnp.where(idv < 0, -1, rid)
    slot_l, rank_l = lane >> 1, lane & 1
    hit, wsum = jnp.zeros((8, 128), f32), jnp.zeros((8, 128), f32)
    for k in range(ids.shape[1]):
        m = rid[:, k : k + 1] == slot_l
        hit = jnp.where(m, 1.0, hit)
        wsum = jnp.where(m, ewv[:, k : k + 1], wsum)
    rank = jnp.zeros((8, 128), f32)
    for s in range(seqs):
        rank += jnp.where(row8 > s, hit[s : s + 1, :], 0.0)
    place = jnp.where(rank == rank_l.astype(f32), hit, 0.0)
    comb = place * wsum
    comb_hi = comb.astype(bf16)
    comb_lo = (comb - comb_hi.astype(f32)).astype(bf16)
    comb2 = jnp.concatenate([comb_hi.astype(f32), comb_lo.astype(f32)], axis=0).astype(bf16)
    place_t = jnp.concatenate([place, jnp.zeros((120, 128), f32)], axis=0).T.astype(bf16)
    done(c_dn)
    for i in range(width // 128):
        cols = pl.ds(128 * i, 128)
        chunk = dcat[:, cols].astype(f32).T.astype(bf16)
        at = 128 * i
        while at < 128 * (i + 1):
            t, o = at // SLOT, at % SLOT
            n = min(SLOT - o, 128 * (i + 1) - at)
            dnt[t, pl.ds(o, n), :] = chunk[at - 128 * i : at - 128 * i + n]
            at += n
    mg = mgain_v[...].astype(f32).reshape(1, width)
    for i in range(width // 128):
        gainb[pl.ds(128 * i, 128), :] = jnp.broadcast_to(mg[:, 128 * i : 128 * (i + 1)], (128, 128)).T

    own_part = send1[pair].astype(f32)
    own_tok = tokblk[pair]
    pltpu.make_async_copy(recv1, recv1, rsem.at[0]).wait()
    attn = own_part + jnp.sum(recv1[...].astype(f32), axis=0)
    lane2 = lax.broadcasted_iota(i32, (8, PAIR), 1)
    mixed = jnp.where(lane2 < 2 * SLOT, own_tok + attn, 0.0).astype(bf16)
    mixed_f = mixed.astype(f32)

    mixed_p = jnp.concatenate([mixed_f, jnp.zeros((120, PAIR), f32)], axis=0).astype(bf16)
    rows = mm(place_t, mixed_p)[0 : 2 * n_ep].astype(bf16)
    send2[...] = rows.reshape(n_ep, 2, PAIR)

    for slot in slots:
        pltpu.make_async_remote_copy(
            src_ref=send2.at[slot], dst_ref=recv2.at[slot], send_sem=ssem.at[1], recv_sem=rsem.at[1],
            device_id={"ep": ep_at(slot)}, device_id_type=MESH).start()
    recv2[0] = send2[0]
    done(c_wt)
    w_copy = pltpu.make_async_remote_copy(
        src_ref=wt.at[pl.ds(0, 256)], dst_ref=wt.at[pl.ds(256, 256)], send_sem=wsem.at[0], recv_sem=wsem.at[1],
        device_id=sibling, device_id_type=MESH)
    w_copy.start()
    for v in range(n_y):
        pltpu.make_async_remote_copy(
            src_ref=dnt.at[v * 2 + 1 - c], dst_ref=dsib.at[v], send_sem=wsem.at[2], recv_sem=wsem.at[3],
            device_id=sibling, device_id_type=MESH).start()
    pltpu.make_async_copy(recv2.at[pl.ds(1, n_ep - 1)], recv2.at[pl.ds(1, n_ep - 1)], rsem.at[1]).wait()
    got = recv2[...].reshape(2 * n_ep, PAIR).astype(f32)
    rows_t = jnp.concatenate([got, mixed_f, jnp.zeros((120 - 2 * n_ep, PAIR), f32)], axis=0).T.astype(bf16)
    for hi in range(2):
        xt[pair + half * hi, pl.ds(0, 128), :] = rows_t[128 * hi : 128 * hi + 128]
        xt[pair + half * hi, pl.ds(128, REST), :] = rows_t[256 + REST * hi : 256 + REST * (hi + 1)]

    moves = [(2, 0), (n_y - 2, 0), (1, 0), (n_y - 1, 0), (1, half), (n_y - 1, half)]

    def gather_copy(k):
        dy, off = moves[k]
        t = lax.rem(me_tp + off, n_tp)
        return pltpu.make_async_remote_copy(
            src_ref=xt.at[t], dst_ref=xt.at[t], send_sem=s3.at[k], recv_sem=r3.at[k],
            device_id={"tp": lax.rem(me_tp + 2 * dy, n_tp)}, device_id_type=MESH)

    def hand_copy(k):
        if k < len(moves):
            dy, off = moves[k]
            t = lax.rem(me_tp + 2 * (n_y - dy) + off, n_tp)
        else:
            t = (me_tp, other)[k - len(moves)]
        return pltpu.make_async_remote_copy(
            src_ref=xt.at[t], dst_ref=xt.at[t], send_sem=f3s.at[k], recv_sem=f3r.at[k],
            device_id=sibling, device_id_type=MESH)

    for k in range(len(moves)):
        gather_copy(k).start()
    hand_copy(len(moves)).start()
    hand_copy(len(moves) + 1).start()
    for k in (2, 3, 4, 5, 0, 1):
        gather_copy(k).wait_recv()
        hand_copy(k).start()
    pltpu.make_async_copy(wt.at[pl.ds(256, 256)], wt.at[pl.ds(256, 256)], wsem.at[1]).wait()
    pltpu.make_async_copy(dsib, dsib, wsem.at[3]).wait()
    for k in range(len(moves) + 2):
        hand_copy(k).wait_recv()

    xa = xt[...].reshape(width, 128).astype(f32)
    inv_rms = lax.rsqrt(jnp.sum(xa * xa, axis=0, keepdims=True) * (1.0 / width) + EPS)
    xn = (xa * inv_rms * gainb[...]).astype(bf16)
    hid = mm(wt[...], xn)
    routed_l = lax.broadcasted_iota(i32, (64, 128), 1) < 2 * n_ep
    parts = []
    for o in (0, 256):
        ge, ue, gs, us = (hid[o + 64 * i : o + 64 * (i + 1)] for i in range(4))
        parts.append(jnp.where(routed_l, ge / (1.0 + jnp.exp(-ge)) * ue, 0.0))
        parts.append(jnp.where(routed_l, 0.0, gs / (1.0 + jnp.exp(-gs)) * us))
    hcat = jnp.concatenate(parts, axis=0).astype(bf16)

    far = sorted(range(1, n_y), key=lambda d: -min(d, n_y - d))

    def sum_copy(dy):
        v = lax.rem(y + dy, n_y)
        return pltpu.make_async_remote_copy(
            src_ref=q5.at[v], dst_ref=recv5.at[dy], send_sem=s5.at[dy], recv_sem=r5.at[dy],
            device_id={"tp": v * 2 + c}, device_id_type=MESH)

    for dy in far + [0]:
        v = lax.rem(y + dy, n_y)
        term = mm(jnp.concatenate([dnt[v * 2 + c], dsib[v]], axis=1), hcat)
        if dy:
            q5[v] = term.astype(bf16)
            sum_copy(dy).start()
        else:
            total = term
    for dy in reversed(far):
        sum_copy(dy).wait_recv()
        total += recv5[dy].astype(f32)
    back = jnp.concatenate([total, jnp.zeros((LANES - SLOT, 128), f32)], axis=0).T
    shared = back[2 * n_ep : 2 * n_ep + 8]
    send6[...] = back[0 : 2 * n_ep].astype(bf16).reshape(n_ep, 2, LANES)

    for slot in slots:
        pltpu.make_async_remote_copy(
            src_ref=send6.at[slot], dst_ref=recv6.at[slot], send_sem=ssem.at[2], recv_sem=rsem.at[2],
            device_id={"ep": ep_back(slot)}, device_id_type=MESH).start()
    recv6[0] = send6[0]
    pltpu.make_async_copy(recv1, recv1, ssem.at[0]).wait()
    pltpu.make_async_copy(recv2.at[pl.ds(1, n_ep - 1)], recv2.at[pl.ds(1, n_ep - 1)], ssem.at[1]).wait()
    w_copy.wait_send()
    pltpu.make_async_copy(dsib, dsib, wsem.at[2]).wait()
    for k in range(len(moves) + 2):
        hand_copy(k).wait_send()
        if k < len(moves):
            gather_copy(k).wait_send()
    for dy in far:
        sum_copy(dy).wait_send()
    pltpu.make_async_copy(recv6.at[pl.ds(1, n_ep - 1)], recv6.at[pl.ds(1, n_ep - 1)], rsem.at[2]).wait()
    vals = recv6[...].reshape(2 * n_ep, LANES)
    two = mm(comb2[:, 0 : 2 * n_ep], vals)
    hi = y >= n_y // 2
    mine = jnp.concatenate(
        [jnp.where(hi, mixed_f[:, 128:256], mixed_f[:, 0:128]),
         jnp.where(hi, pltpu.roll(mixed_f[:, 256:384], 128 - REST, 1), mixed_f[:, 256:384])], axis=1)
    res = mine + (two[0:8] + two[8:16]) + shared
    out[...] = res[0:seqs, 0:SLOT].astype(bf16)
    pltpu.make_async_copy(recv6.at[pl.ds(1, n_ep - 1)], recv6.at[pl.ds(1, n_ep - 1)], ssem.at[2]).wait()


def solution(mesh):
    n_ep, n_tp = mesh.shape["ep"], mesh.shape["tp"]
    n_y = half = n_tp // 2

    def step(tokens, attn_gain, wq, wk, wv, ow, lambdas, head_gain, ck, cv, lengths, moe_gain,
             gw, uw, dw, sg, su, sd, ids, ew):
        seqs, width = tokens.shape
        cache = ck.shape[1]
        pairs = (seqs + 1) // 2
        V, DMA = pltpu.VMEM, pltpu.SemaphoreType.DMA
        scratch = [
            V((seqs, width), bf16), V((width, 384), bf16), V((pairs, cache, 256), bf16), V((pairs, cache, 256), bf16),
            V((half, PAIR, 128), bf16), V((512, width), bf16), V((128, width), bf16),
            pltpu.SMEM((1,), f32), pltpu.SMEM((seqs,), i32), V((width,), bf16), V((128,), bf16), V((width,), bf16),
            V(ids.shape, i32), V(ew.shape, f32),
            V((8, width), f32), V((half, 8, PAIR), f32), V((8, 128), i32), V((8, 128), f32),
            V((n_tp, SLOT, 128), bf16), V((n_y, SLOT, 128), bf16), V((width, 128), f32),
            V((half, 8, PAIR), bf16), V((n_tp - 1, 8, PAIR), bf16),
            V((n_ep, 2, PAIR), bf16), V((n_ep, 2, PAIR), bf16),
            V((n_tp, SLOT, 128), bf16), V((n_y, SLOT, 128), bf16), V((n_y, SLOT, 128), bf16),
            V((n_ep, 2, LANES), bf16), V((n_ep, 2, LANES), bf16),
            DMA((72,)), DMA((3,)), DMA((3,)),
            DMA((n_y,)), DMA((n_y,)), DMA((n_y,)), DMA((n_y,)), DMA((n_y,)), DMA((n_y,)), DMA((4,)),
        ]
        return pl.pallas_call(
            functools.partial(kernel, n_ep, n_tp),
            out_shape=jax.ShapeDtypeStruct((seqs, width // n_tp), bf16),
            in_specs=[pl.BlockSpec(memory_space=pl.ANY)] * 20,
            out_specs=pl.BlockSpec(memory_space=pltpu.VMEM),
            scratch_shapes=scratch,
            compiler_params=pltpu.CompilerParams(collective_id=0, has_side_effects=True),
            name="decode_step",
        )(tokens, attn_gain, wq, wk, wv, ow, lambdas, head_gain,
          ck.reshape(seqs, cache, 128), cv.reshape(seqs, cache, 128), lengths, moe_gain,
          gw[0].T, uw[0].T, dw[0], sg.T, su.T, sd, ids, ew)

    in_specs = (
        P("ep", None), P(), P(None, "tp"), P(None, "tp"), P(None, "tp"), P(None, "tp"), P("tp"), P(),
        P("ep", None, "tp", None), P("ep", None, "tp", None), P("ep"), P(),
        P("ep", None, "tp"), P("ep", None, "tp"), P("ep", "tp", None),
        P(None, "tp"), P(None, "tp"), P("tp", None), P("ep", None), P("ep", None),
    )
    return jax.shard_map(step, mesh=mesh, in_specs=in_specs, out_specs=P("ep", "tp"), check_vma=False)
```

```python
import functools

import jax
import jax.numpy as jnp
from jax import lax
from jax.experimental import pallas as pl
from jax.experimental.pallas import tpu as pltpu
from jax.sharding import PartitionSpec as P

EPS = 1e-06
NX = 4
MESH = pl.DeviceIdType.MESH
NT = (((1,), (1,)), ((), ()))
bf16, f32, i32 = jnp.bfloat16, jnp.float32, jnp.int32
SLOT = 144
LANES = 256
BLOCK = 2 * SLOT
PAIR = 384
HEADK = 256
TAILK = BLOCK - HEADK


def wrap(v, n):
    return jnp.where(v < 0, v + n, v)


def mm(a, b):
    return jnp.dot(a, b, preferred_element_type=f32)


def mm_nt(a, b):
    return lax.dot_general(a, b, NT, preferred_element_type=f32)


def kernel(
    n_ep, n_tp,
    tok, again, wq, wk, wv, ow, lam, hgain, ck, cv, lens, mgain, gwt, uwt, dw, sgt, sut, sd, ids, ew,
    out,
    tok_v, wqkv, k_v, v_v, ow_v, wt, dcat, lam_v, lens_s, again_v, hgain_v, mgain_v, ids_v, ew_v,
    x_s, tokblk, idp, ewp, dnt, dsib, wp,
    send1, recv1, send2, recv2, xt, q5, recv5, send6, recv6, share_s, share_r,
    lsem, ssem, rsem, r3, f3r, wsem, hsem,
):
    n_z, n_y = n_ep // NX, n_tp // 2
    seqs, width = tok.shape
    cache = ck.shape[1]
    me_ep, me_tp = lax.axis_index("ep"), lax.axis_index("tp")
    z, x = me_ep // NX, lax.rem(me_ep, NX)
    y, c = me_tp // 2, lax.rem(me_tp, 2)

    half = n_tp // 2
    pair = lax.rem(me_tp, half)
    other = lax.rem(me_tp + half, n_tp)
    sibling = {"tp": y * 2 + 1 - c}
    above, below = lax.rem(me_tp + 2, n_tp), lax.rem(me_tp + n_tp - 2, n_tp)
    z_at = [wrap(z + d - n_z, n_z) * NX for d in range(n_z)]
    x_at = [wrap(x + d - NX, NX) for d in range(NX)]

    def hops(slot):
        dz, dx = slot // NX, slot % NX
        return min(dz, n_z - dz) + min(dx, NX - dx)

    slots = sorted(range(1, n_ep), key=lambda s: -hops(s))

    def ep_at(slot):
        return z_at[slot // NX] + x_at[slot % NX]

    def ep_back(slot):
        return z_at[-(slot // NX) % n_z] + x_at[-(slot % NX) % NX]

    bar = pltpu.get_barrier_semaphore()
    groups = []

    def load(pairs, region=None):
        sem = lsem.at[len(groups)]
        for src, dst in pairs:
            pltpu.make_async_copy(src, dst, sem).start()
        groups.append(region)
        region = pairs[0][1] if region is None else region
        return lambda: whole(region, sem)

    def whole(ref, sem):
        pltpu.make_async_copy(ref, ref, sem).wait()

    def cached(src, dst):
        return [
            load([(src.at[s], dst.at[p, :, pl.ds(128 * (s % 2), 128)]) for s in range(2 * p, min(2 * p + 2, seqs))],
                 dst.at[p, :, pl.ds(0, 128 * min(2, seqs - 2 * p))])
            for p in range((seqs + 1) // 2)]

    c_tok, c_gain = load([(tok, tok_v)]), load([(again, again_v)])
    step = width // 3
    c_qkv = [
        load([(w.at[pl.ds(step * j, step)], wqkv.at[pl.ds(step * j, step), pl.ds(128 * i, 128)])
              for i, w in enumerate((wq, wk, wv))], wqkv.at[pl.ds(step * j, step)])
        for j in range(3)]
    for slot in slots:
        pl.semaphore_signal(bar, inc=1, device_id={"ep": ep_at(slot), "tp": above}, device_id_type=MESH)
        pl.semaphore_signal(bar, inc=1, device_id={"ep": ep_at(slot)}, device_id_type=MESH)
    for r in range(1, n_tp):
        pl.semaphore_signal(bar, inc=1, device_id={"tp": lax.rem(me_tp + r, n_tp)}, device_id_type=MESH)
    c_k = cached(ck, k_v)
    c_len, c_lam, c_hgain = load([(lens, lens_s)]), load([(lam, lam_v)]), load([(hgain, hgain_v)])
    c_v = cached(cv, v_v)
    c_ow = load(
        [(ow.at[pl.ds(SLOT * t, SLOT)], ow_v.at[t % half, pl.ds(SLOT * (t // half), SLOT)]) for t in range(n_tp)],
        ow_v.at[:, pl.ds(0, BLOCK)])
    c_ids, c_ew, c_mgain = load([(ids, ids_v)]), load([(ew, ew_v)]), load([(mgain, mgain_v)])
    c_dn = load([(w, dcat.at[pl.ds(64 * i, 64)]) for i, w in enumerate((dw, sd))], dcat)
    c_wt = load([(w, wt.at[pl.ds(64 * i, 64)]) for i, w in enumerate((gwt, uwt, sgt, sut))], wt)

    x_s[...] = jnp.zeros_like(x_s)
    if seqs % 2:
        k_v[seqs // 2, :, pl.ds(128, 128)] = jnp.zeros((cache, 128), bf16)
        v_v[seqs // 2, :, pl.ds(128, 128)] = jnp.zeros((cache, 128), bf16)
    c_tok()
    c_gain()
    x_s[0:seqs, :] = tok_v[...].astype(f32)
    xv = x_s[...]
    gain = again_v[...].astype(f32).reshape(1, width)
    normed = (xv * lax.rsqrt(jnp.mean(xv * xv, axis=-1, keepdims=True) + EPS) * gain).astype(bf16)
    qkv = jnp.zeros((8, 384), f32)
    for j in range(3):
        c_qkv[j]()
        qkv += mm(normed[:, step * j : step * (j + 1)], wqkv[pl.ds(step * j, step), :])
    qkv = qkv.astype(bf16).astype(f32)
    q, kn, vn = qkv[:, 0:128], qkv[:, 128:256], qkv[:, 256:384]
    lane = lax.broadcasted_iota(i32, (8, 128), 1)
    first = lane < 64
    qk = q * kn
    scale = 0.125
    own = jnp.concatenate(
        [jnp.sum(jnp.where(first, qk, 0.0), axis=-1, keepdims=True),
         jnp.sum(jnp.where(first, 0.0, qk), axis=-1, keepdims=True)], axis=0) * scale
    q2 = jnp.concatenate([jnp.where(first, q, 0.0), jnp.where(first, 0.0, q)], axis=0)
    row16 = lax.broadcasted_iota(i32, (16, 128), 0)
    row16 = jnp.where(row16 >= 8, row16 - 8, row16)
    scores = jnp.zeros((16, cache), f32)
    c_len()
    c_lam()
    c_hgain()
    for p in range((seqs + 1) // 2):
        c_k[p]()
        qa = jnp.where(row16 == 2 * p, q2, 0.0)
        qb = jnp.where(row16 == 2 * p + 1, q2, 0.0)
        scores += mm_nt(jnp.concatenate([qa, qb], axis=1).astype(bf16), k_v[p])
    scores = scores * scale
    rcol = lax.broadcasted_iota(i32, (16, 1), 0)
    rcol = jnp.where(rcol >= 8, rcol - 8, rcol)
    lcol = jnp.zeros((16, 1), i32)
    for s in range(seqs):
        lcol = jnp.where(rcol == s, lens_s[s], lcol)
    live = lax.broadcasted_iota(i32, (16, cache), 1) < lcol
    peak = jnp.maximum(jnp.max(jnp.where(live, scores, -jnp.inf), axis=-1, keepdims=True), own)
    terms = jnp.where(live, jnp.exp(scores - peak), 0.0)
    own_term = jnp.exp(own - peak)
    inv = 1.0 / (jnp.sum(terms, axis=-1, keepdims=True) + own_term)
    probs, own_prob = terms * inv, own_term * inv
    lm = lam_v[...]
    mix = (probs[0:8] - lm * probs[8:16]).astype(bf16).astype(f32)
    own_mix = (own_prob[0:8] - lm * own_prob[8:16]).astype(bf16).astype(f32)
    rowc = lax.broadcasted_iota(i32, (8, cache), 0)
    both = jnp.zeros((8, 256), f32)
    for p in range((seqs + 1) // 2):
        c_v[p]()
        both += mm(jnp.where(rowc // 2 == p, mix, 0.0).astype(bf16), v_v[p])
    row8 = lax.broadcasted_iota(i32, (8, 128), 0)
    head = jnp.where(row8 % 2 == 0, both[:, 0:128], both[:, 128:256]) + own_mix * vn
    hg = hgain_v[...].astype(f32).reshape(1, 128)
    head_n = (head * lax.rsqrt(jnp.mean(head * head, axis=-1, keepdims=True) + EPS) * hg).astype(bf16)
    c_ow()
    part = mm_nt(head_n, ow_v[...].reshape(half * PAIR, 128)).astype(bf16)
    for p in range(half):
        send1[p] = part[:, PAIR * p : PAIR * (p + 1)]

    pl.semaphore_wait(bar, n_tp - 1 + 2 * (n_ep - 1))
    for r in sorted(range(1, n_tp), key=lambda r: -min(r, n_tp - r)):
        to = lax.rem(me_tp + r, n_tp)
        pltpu.make_async_remote_copy(
            src_ref=send1.at[lax.rem(to, half)], dst_ref=recv1.at[r - 1], send_sem=ssem.at[0], recv_sem=rsem.at[0],
            device_id={"tp": to}, device_id_type=MESH).start()

    for p in range(half):
        q0, q1 = SLOT * p, SLOT * (p + half)
        tokblk[p] = jnp.concatenate(
            [xv[:, q0 : q0 + SLOT], xv[:, q1 : q1 + SLOT], jnp.zeros((8, PAIR - BLOCK), f32)], axis=1)
    c_ids()
    c_ew()
    c_mgain()
    idp[...] = jnp.full_like(idp, -1)
    ewp[...] = jnp.zeros_like(ewp)
    idp[0:seqs, 0 : ids.shape[1]] = ids_v[...]
    ewp[0:seqs, 0 : ids.shape[1]] = ew_v[...]
    idv, ewv = idp[...], ewp[...]
    rid = wrap((idv >> 2) - z, n_z) * NX + wrap((idv & 3) - x, NX)
    rid = jnp.where(idv < 0, -1, rid)
    slot_l, rank_l = lane >> 1, lane & 1
    hit, wsum = jnp.zeros((8, 128), f32), jnp.zeros((8, 128), f32)
    for k in range(ids.shape[1]):
        m = rid[:, k : k + 1] == slot_l
        hit = jnp.where(m, 1.0, hit)
        wsum = jnp.where(m, ewv[:, k : k + 1], wsum)
    rank = jnp.zeros((8, 128), f32)
    for s in range(seqs):
        rank += jnp.where(row8 > s, hit[s : s + 1, :], 0.0)
    place = jnp.where(rank == rank_l.astype(f32), hit, 0.0)
    comb = place * wsum
    comb_hi = comb.astype(bf16)
    comb_lo = (comb - comb_hi.astype(f32)).astype(bf16)
    comb2 = jnp.concatenate([comb_hi.astype(f32), comb_lo.astype(f32)], axis=0).astype(bf16)
    place_t = jnp.concatenate([place, jnp.zeros((120, 128), f32)], axis=0).T.astype(bf16)
    c_dn()
    for i in range(width // 128):
        cols = pl.ds(128 * i, 128)
        chunk = dcat[:, cols].astype(f32).T.astype(bf16)
        at = 128 * i
        while at < 128 * (i + 1):
            t, o = at // SLOT, at % SLOT
            n = min(SLOT - o, 128 * (i + 1) - at)
            dnt[t, pl.ds(o, n), :] = chunk[at - 128 * i : at - 128 * i + n]
            at += n
    mg = mgain_v[...].astype(f32).reshape(1, width)
    c_wt()
    for i in range(4):
        rows = pl.ds(64 * i, 64)
        w = wt[rows, :].astype(f32) * mg
        tails = []
        for p in range(half):
            q0, q1 = SLOT * p, SLOT * (p + half)
            wp[p, rows, :] = jnp.concatenate(
                [w[:, q0 : q0 + SLOT], w[:, q1 : q1 + HEADK - SLOT]], axis=1).astype(bf16)
            tails.append(w[:, q1 + HEADK - SLOT : q1 + SLOT])
        wp[half, rows, :] = jnp.concatenate(tails, axis=1).astype(bf16)
    own_part = send1[pair].astype(f32)
    own_tok = tokblk[pair]
    whole(recv1, rsem.at[0])
    attn = own_part + jnp.sum(recv1[...].astype(f32), axis=0)
    lane2 = lax.broadcasted_iota(i32, (8, PAIR), 1)
    mixed = jnp.where(lane2 < BLOCK, own_tok + attn, 0.0).astype(bf16)
    mixed_f = mixed.astype(f32)

    mixed_p = jnp.concatenate([mixed_f, jnp.zeros((120, PAIR), f32)], axis=0).astype(bf16)
    rows = mm(place_t, mixed_p)[0 : 2 * n_ep].astype(bf16)
    send2[...] = rows.reshape(n_ep, 2, PAIR)

    for slot in slots:
        pltpu.make_async_remote_copy(
            src_ref=send2.at[slot], dst_ref=recv2.at[slot], send_sem=ssem.at[1], recv_sem=rsem.at[1],
            device_id={"ep": ep_at(slot)}, device_id_type=MESH).start()
    recv2[0] = send2[0]
    w_copy = pltpu.make_async_remote_copy(
        src_ref=wp.at[:, pl.ds(0, 256)], dst_ref=wp.at[:, pl.ds(256, 256)], send_sem=wsem.at[0],
        recv_sem=wsem.at[1], device_id=sibling, device_id_type=MESH)
    w_copy.start()
    for v in range(n_y):
        pltpu.make_async_remote_copy(
            src_ref=dnt.at[v * 2 + 1 - c], dst_ref=dsib.at[v], send_sem=wsem.at[2], recv_sem=wsem.at[3],
            device_id=sibling, device_id_type=MESH).start()
    pltpu.make_async_copy(recv2.at[pl.ds(1, n_ep - 1)], recv2.at[pl.ds(1, n_ep - 1)], rsem.at[1]).wait()
    got = recv2[...].reshape(2 * n_ep, PAIR).astype(f32)
    rows_t = jnp.concatenate([got, mixed_f, jnp.zeros((120 - 2 * n_ep, PAIR), f32)], axis=0).T
    xt[pair] = rows_t[0:BLOCK].astype(bf16)

    upper = y // (n_y // 2)

    moves = (2, n_y - 2, 1, n_y - 1)
    hands = moves + (0,)

    def pair_at(dy, core):
        return lax.rem(y + dy, n_y // 2) * 2 + core

    def gather_copy(dy):
        if dy in (1, n_y - 1):
            part = xt.at[pair]
        else:
            part = xt.at[pair, pl.ds(pl.multiple_of(upper * SLOT, 16), SLOT)]
        return pltpu.make_async_remote_copy(
            src_ref=part, dst_ref=part, send_sem=ssem.at[4], recv_sem=r3.at[moves.index(dy)],
            device_id={"tp": lax.rem(me_tp + 2 * dy, n_tp)}, device_id_type=MESH)

    def hand_copy(dy):
        from_y = lax.rem(y + n_y - dy, n_y)
        if dy in (0, 1, n_y - 1):
            part = xt.at[pair_at(n_y - dy, c)]
        else:
            part = xt.at[pair_at(n_y - dy, c), pl.ds(pl.multiple_of(from_y // (n_y // 2) * SLOT, 16), SLOT)]
        return pltpu.make_async_remote_copy(
            src_ref=part, dst_ref=part, send_sem=ssem.at[5], recv_sem=f3r.at[hands.index(dy)],
            device_id=sibling, device_id_type=MESH)

    def products(dy, core):
        p = pair_at(n_y - dy, core)
        block = xt[p]
        wide = block.astype(f32)
        return mm(wp[p], block[0:HEADK]), jnp.sum(wide * wide, axis=0, keepdims=True)

    for dy in moves:
        gather_copy(dy).start()
    hand_copy(0).start()
    pltpu.make_async_copy(wp.at[:, pl.ds(256, 256)], wp.at[:, pl.ds(256, 256)], wsem.at[1]).wait()
    hid, squares = products(0, c)
    for dy in (1, n_y - 1):
        gather_copy(dy).wait_recv()
        hand_copy(dy).start()
    for dy in (1, n_y - 1):
        more = products(dy, c)
        hid, squares = hid + more[0], squares + more[1]
    hand_copy(0).wait_recv()
    more = products(0, 1 - c)
    hid, squares = hid + more[0], squares + more[1]
    for dy in (2, n_y - 2):
        gather_copy(dy).wait_recv()
        hand_copy(dy).start()
    more = products(2, c)
    hid, squares = hid + more[0], squares + more[1]
    for dy in (1, n_y - 1):
        hand_copy(dy).wait_recv()
        more = products(dy, 1 - c)
        hid, squares = hid + more[0], squares + more[1]
    whole(dsib, wsem.at[3])
    for dy in (2, n_y - 2):
        hand_copy(dy).wait_recv()
    more = products(2, 1 - c)
    hid, squares = hid + more[0], squares + more[1]
    tails = jnp.concatenate([xt[p, pl.ds(HEADK, TAILK), :] for p in range(half)], axis=0)
    hid = (hid + mm(wp[half], tails)) * lax.rsqrt(squares * (1.0 / width) + EPS)
    routed_l = lax.broadcasted_iota(i32, (64, 128), 1) < 2 * n_ep
    parts = []
    for o in (0, 256):
        ge, ue, gs, us = (hid[o + 64 * i : o + 64 * (i + 1)] for i in range(4))
        parts.append(jnp.where(routed_l, ge / (1.0 + jnp.exp(-ge)) * ue, 0.0))
        parts.append(jnp.where(routed_l, 0.0, gs / (1.0 + jnp.exp(-gs)) * us))
    hcat = jnp.concatenate(parts, axis=0).astype(bf16)

    far = (3, n_y - 3, 2, n_y - 2, 1, n_y - 1)
    far_at = {dy: i for i, dy in enumerate(far)}

    def sum_copy(dy):
        to = lax.rem(y + dy, n_y)
        v = to if dy < n_y // 2 else lax.rem(to + n_y - 1, n_y)
        return pltpu.make_async_remote_copy(
            src_ref=q5.at[v], dst_ref=recv5.at[far_at[dy]], send_sem=ssem.at[6], recv_sem=rsem.at[4],
            device_id={"tp": to * 2 + c}, device_id_type=MESH)

    def terms(v):
        return mm(jnp.concatenate([dnt[v * 2 + c], dsib[v]], axis=1), hcat)

    for dy in far:
        to = lax.rem(y + dy, n_y)
        v = to if dy < n_y // 2 else lax.rem(to + n_y - 1, n_y)
        q5[v] = terms(v).astype(bf16)
        sum_copy(dy).start()
    totals = [terms(y), terms(lax.rem(y + n_y - 1, n_y))]
    whole(recv5, rsem.at[4])
    for dy in far:
        side = 0 if dy < n_y // 2 else 1
        totals[side] += recv5[far_at[dy]].astype(f32)
    backs = [jnp.concatenate([a, jnp.zeros((LANES - SLOT, 128), f32)], axis=0).T for a in totals]
    shared = backs[0][2 * n_ep : 2 * n_ep + 8]
    share_s[...] = backs[1][2 * n_ep : 2 * n_ep + 8]
    for side in range(2):
        send6[side] = backs[side][0 : 2 * n_ep].astype(bf16).reshape(n_ep, 2, LANES)

    for slot in slots + [0]:
        for side in (1, 0) if slot else (1,):
            pltpu.make_async_remote_copy(
                src_ref=send6.at[side, slot], dst_ref=recv6.at[side, slot],
                send_sem=ssem.at[2 + side], recv_sem=rsem.at[2 + side],
                device_id={"ep": ep_back(slot), "tp": below if side else me_tp}, device_id_type=MESH).start()
    share_copy = pltpu.make_async_remote_copy(
        src_ref=share_s, dst_ref=share_r, send_sem=hsem.at[0], recv_sem=hsem.at[1],
        device_id={"tp": below}, device_id_type=MESH)
    share_copy.start()
    recv6[0, 0] = send6[0, 0]
    whole(recv1, ssem.at[0])
    pltpu.make_async_copy(recv2.at[pl.ds(1, n_ep - 1)], recv2.at[pl.ds(1, n_ep - 1)], ssem.at[1]).wait()
    w_copy.wait_send()
    whole(dsib, wsem.at[2])
    whole(xt.at[pl.ds(0, 3)], ssem.at[4])
    whole(xt.at[pl.ds(0, 4)], ssem.at[5])
    whole(recv5, ssem.at[6])
    share_copy.wait_recv()
    whole(recv6.at[0, pl.ds(1, n_ep - 1)], rsem.at[2])
    whole(recv6.at[1], rsem.at[3])
    shared = shared + share_r[...]
    two = sum(mm(comb2[:, 0 : 2 * n_ep], recv6[side].reshape(2 * n_ep, LANES)) for side in range(2))
    mine = jnp.where(y >= n_y // 2, mixed_f[:, SLOT : BLOCK], mixed_f[:, 0:SLOT])
    res = mine + ((two[0:8] + two[8:16]) + shared)[:, 0:SLOT]
    out[...] = res[0:seqs].astype(bf16)
    whole(recv6.at[0, pl.ds(1, n_ep - 1)], ssem.at[2])
    whole(recv6.at[1], ssem.at[3])
    share_copy.wait_send()


def solution(mesh):
    n_ep, n_tp = mesh.shape["ep"], mesh.shape["tp"]
    n_y = half = n_tp // 2

    def step(tokens, attn_gain, wq, wk, wv, ow, lambdas, head_gain, ck, cv, lengths, moe_gain,
             gw, uw, dw, sg, su, sd, ids, ew):
        seqs, width = tokens.shape
        cache = ck.shape[1]
        pairs = (seqs + 1) // 2
        V, DMA = pltpu.VMEM, pltpu.SemaphoreType.DMA
        scratch = [
            V((seqs, width), bf16), V((width, 384), bf16), V((pairs, cache, 256), bf16), V((pairs, cache, 256), bf16),
            V((half, PAIR, 128), bf16), V((256, width), bf16), V((128, width), bf16),
            V((1, 1), f32), pltpu.SMEM((seqs,), i32), V((width,), bf16), V((128,), bf16), V((width,), bf16),
            V(ids.shape, i32), V(ew.shape, f32),
            V((8, width), f32), V((half, 8, PAIR), f32), V((8, 128), i32), V((8, 128), f32),
            V((n_tp, SLOT, 128), bf16), V((n_y, SLOT, 128), bf16), V((half + 1, 512, HEADK), bf16),
            V((half, 8, PAIR), bf16), V((n_tp - 1, 8, PAIR), bf16),
            V((n_ep, 2, PAIR), bf16), V((n_ep, 2, PAIR), bf16),
            V((half, BLOCK, 128), bf16), V((n_y, SLOT, 128), bf16), V((n_y - 2, SLOT, 128), bf16),
            V((2, n_ep, 2, LANES), bf16), V((2, n_ep, 2, LANES), bf16), V((8, LANES), f32), V((8, LANES), f32),
            DMA((24,)), DMA((7,)), DMA((5,)), DMA((4,)), DMA((5,)), DMA((4,)), DMA((2,)),
        ]
        return pl.pallas_call(
            functools.partial(kernel, n_ep, n_tp),
            out_shape=pltpu.VMEM((seqs, width // n_tp), bf16),
            in_specs=[pl.BlockSpec(memory_space=pl.ANY)] * 20,
            out_specs=pl.BlockSpec(memory_space=pltpu.VMEM),
            scratch_shapes=scratch,
            compiler_params=pltpu.CompilerParams(collective_id=0, has_side_effects=True),
            name="decode_step",
        )(tokens, attn_gain, wq, wk, wv, ow, lambdas.reshape(1, 1), head_gain,
          ck.reshape(seqs, cache, 128), cv.reshape(seqs, cache, 128), lengths, moe_gain,
          gw[0].T, uw[0].T, dw[0], sg.T, su.T, sd, ids, ew)

    in_specs = (
        P("ep", None), P(), P(None, "tp"), P(None, "tp"), P(None, "tp"), P(None, "tp"), P("tp"), P(),
        P("ep", None, "tp", None), P("ep", None, "tp", None), P("ep"), P(),
        P("ep", None, "tp"), P("ep", None, "tp"), P("ep", "tp", None),
        P(None, "tp"), P(None, "tp"), P("tp", None), P("ep", None), P("ep", None),
    )
    return jax.shard_map(step, mesh=mesh, in_specs=in_specs, out_specs=P("ep", "tp"), check_vma=False)
```

```python
import functools

import jax
import jax.numpy as jnp
from jax import lax
from jax.experimental import pallas as pl
from jax.experimental.pallas import tpu as pltpu
from jax.sharding import PartitionSpec as P

EPS = 1e-06
NX = 4
MESH = pl.DeviceIdType.MESH
NT = (((1,), (1,)), ((), ()))
bf16, f32, i32 = jnp.bfloat16, jnp.float32, jnp.int32
SLOT = 144
LANES = 256
BLOCK = 2 * SLOT
PAIR = 384
FOLD = 120
HEADK = 256
TAILK = BLOCK - HEADK


def wrap(v, n):
    return jnp.where(v < 0, v + n, v)


def mm(a, b):
    return jnp.dot(a, b, preferred_element_type=f32)


def mm_nt(a, b):
    return lax.dot_general(a, b, NT, preferred_element_type=f32)


def kernel(
    n_ep, n_tp,
    tok, again, wq, wk, wv, ow, lam, hgain, ck, cv, lens, mgain, gwt, uwt, dw, sgt, sut, sd, ids, ew,
    out,
    tok_v, wqkv, k_v, v_v, ow_v, wt, dcat, lam_v, lens_s, again_v, hgain_v, mgain_v, ids_v, ew_v,
    x_s, tokblk, idp, ewp, dnt, drem, dsib, dsibr, wp,
    send1, recv1, send2, recv2, xt, q5, recv5, send6, recv6, share_s, share_r,
    lsem, ssem, rsem, r3, f3r, wsem, hsem,
):
    n_z, n_y = n_ep // NX, n_tp // 2
    seqs, width = tok.shape
    cache = ck.shape[1]
    me_ep, me_tp = lax.axis_index("ep"), lax.axis_index("tp")
    z, x = me_ep // NX, lax.rem(me_ep, NX)
    y, c = me_tp // 2, lax.rem(me_tp, 2)

    half = n_tp // 2
    pair = lax.rem(me_tp, half)
    other = lax.rem(me_tp + half, n_tp)
    sibling = {"tp": y * 2 + 1 - c}
    below = lax.rem(me_tp + n_tp - 2, n_tp)
    z_at = [wrap(z + d - n_z, n_z) * NX for d in range(n_z)]
    x_at = [wrap(x + d - NX, NX) for d in range(NX)]

    def hops(slot):
        dz, dx = slot // NX, slot % NX
        return min(dz, n_z - dz) + min(dx, NX - dx)

    slots = sorted(range(1, n_ep), key=lambda s: -hops(s))

    def ep_at(slot):
        return z_at[slot // NX] + x_at[slot % NX]

    def ep_back(slot):
        return z_at[-(slot // NX) % n_z] + x_at[-(slot % NX) % NX]

    bar = pltpu.get_barrier_semaphore()
    groups = []

    def load(pairs, region=None):
        sem = lsem.at[len(groups)]
        for src, dst in pairs:
            pltpu.make_async_copy(src, dst, sem).start()
        groups.append(region)
        region = pairs[0][1] if region is None else region
        return lambda: whole(region, sem)

    def whole(ref, sem):
        pltpu.make_async_copy(ref, ref, sem).wait()

    def cached(src, dst):
        return [
            load([(src.at[s], dst.at[p, :, pl.ds(128 * (s % 2), 128)]) for s in range(2 * p, min(2 * p + 2, seqs))],
                 dst.at[p, :, pl.ds(0, 128 * min(2, seqs - 2 * p))])
            for p in range((seqs + 1) // 2)]

    for slot in slots:
        pl.semaphore_signal(bar, inc=1, device_id={"ep": ep_at(slot)}, device_id_type=MESH)
    for r in range(1, n_tp):
        pl.semaphore_signal(bar, inc=1, device_id={"tp": lax.rem(me_tp + r, n_tp)}, device_id_type=MESH)
    c_tok, c_gain = load([(tok, tok_v)]), load([(again, again_v)])
    step = width // 3
    c_qkv = [
        load([(w.at[pl.ds(step * j, step)], wqkv.at[pl.ds(step * j, step), pl.ds(128 * i, 128)])
              for i, w in enumerate((wq, wk, wv))], wqkv.at[pl.ds(step * j, step)])
        for j in range(3)]
    c_k = cached(ck, k_v)
    c_len, c_lam, c_hgain = load([(lens, lens_s)]), load([(lam, lam_v)]), load([(hgain, hgain_v)])
    c_v = cached(cv, v_v)
    c_ow = load(
        [(ow.at[pl.ds(SLOT * t, SLOT)], ow_v.at[t % half, pl.ds(SLOT * (t // half), SLOT)]) for t in range(n_tp)],
        ow_v.at[:, pl.ds(0, BLOCK)])
    c_ids, c_ew, c_mgain = load([(ids, ids_v)]), load([(ew, ew_v)]), load([(mgain, mgain_v)])
    c_dn = load([(w, dcat.at[pl.ds(64 * i, 64)]) for i, w in enumerate((dw, sd))], dcat)
    c_wt = load([(w, wt.at[pl.ds(64 * i, 64)]) for i, w in enumerate((gwt, uwt, sgt, sut))], wt)

    x_s[...] = jnp.zeros_like(x_s)
    if seqs % 2:
        k_v[seqs // 2, :, pl.ds(128, 128)] = jnp.zeros((cache, 128), bf16)
        v_v[seqs // 2, :, pl.ds(128, 128)] = jnp.zeros((cache, 128), bf16)
    c_tok()
    c_gain()
    x_s[0:seqs, :] = tok_v[...].astype(f32)
    xv = x_s[...]
    gain = again_v[...].astype(f32).reshape(1, width)
    normed = (xv * lax.rsqrt(jnp.mean(xv * xv, axis=-1, keepdims=True) + EPS) * gain).astype(bf16)
    qkv = jnp.zeros((8, 384), f32)
    for j in range(3):
        c_qkv[j]()
        qkv += mm(normed[:, step * j : step * (j + 1)], wqkv[pl.ds(step * j, step), :])
    qkv = qkv.astype(bf16).astype(f32)
    q, kn, vn = qkv[:, 0:128], qkv[:, 128:256], qkv[:, 256:384]
    lane = lax.broadcasted_iota(i32, (8, 128), 1)
    first = lane < 64
    qk = q * kn
    scale = 0.125
    own = jnp.concatenate(
        [jnp.sum(jnp.where(first, qk, 0.0), axis=-1, keepdims=True),
         jnp.sum(jnp.where(first, 0.0, qk), axis=-1, keepdims=True)], axis=0) * scale
    q2 = jnp.concatenate([jnp.where(first, q, 0.0), jnp.where(first, 0.0, q)], axis=0)
    row16 = lax.broadcasted_iota(i32, (16, 128), 0)
    row16 = jnp.where(row16 >= 8, row16 - 8, row16)
    scores = jnp.zeros((16, cache), f32)
    c_len()
    c_lam()
    c_hgain()
    for p in range((seqs + 1) // 2):
        c_k[p]()
        qa = jnp.where(row16 == 2 * p, q2, 0.0)
        qb = jnp.where(row16 == 2 * p + 1, q2, 0.0)
        scores += mm_nt(jnp.concatenate([qa, qb], axis=1).astype(bf16), k_v[p])
    scores = scores * scale
    rcol = lax.broadcasted_iota(i32, (16, 1), 0)
    rcol = jnp.where(rcol >= 8, rcol - 8, rcol)
    lcol = jnp.zeros((16, 1), i32)
    for s in range(seqs):
        lcol = jnp.where(rcol == s, lens_s[s], lcol)
    live = lax.broadcasted_iota(i32, (16, cache), 1) < lcol
    peak = jnp.maximum(jnp.max(jnp.where(live, scores, -jnp.inf), axis=-1, keepdims=True), own)
    terms = jnp.where(live, jnp.exp(scores - peak), 0.0)
    own_term = jnp.exp(own - peak)
    inv = 1.0 / (jnp.sum(terms, axis=-1, keepdims=True) + own_term)
    probs, own_prob = terms * inv, own_term * inv
    lm = lam_v[...]
    mix = (probs[0:8] - lm * probs[8:16]).astype(bf16).astype(f32)
    own_mix = (own_prob[0:8] - lm * own_prob[8:16]).astype(bf16).astype(f32)
    rowc = lax.broadcasted_iota(i32, (8, cache), 0)
    both = jnp.zeros((8, 256), f32)
    for p in range((seqs + 1) // 2):
        c_v[p]()
        both += mm(jnp.where(rowc // 2 == p, mix, 0.0).astype(bf16), v_v[p])
    row8 = lax.broadcasted_iota(i32, (8, 128), 0)
    head = jnp.where(row8 % 2 == 0, both[:, 0:128], both[:, 128:256]) + own_mix * vn
    hg = hgain_v[...].astype(f32).reshape(1, 128)
    head_n = (head * lax.rsqrt(jnp.mean(head * head, axis=-1, keepdims=True) + EPS) * hg).astype(bf16)
    c_ow()
    part = mm_nt(head_n, ow_v[...].reshape(half * PAIR, 128)).astype(bf16)
    for p in range(half):
        send1[p] = part[:, PAIR * p : PAIR * (p + 1)]

    pl.semaphore_wait(bar, n_tp - 1 + n_ep - 1)
    for r in sorted(range(1, n_tp), key=lambda r: -min(r, n_tp - r)):
        to = lax.rem(me_tp + r, n_tp)
        pltpu.make_async_remote_copy(
            src_ref=send1.at[lax.rem(to, half)], dst_ref=recv1.at[r - 1], send_sem=ssem.at[0], recv_sem=rsem.at[0],
            device_id={"tp": to}, device_id_type=MESH).start()

    for p in range(half):
        q0, q1 = SLOT * p, SLOT * (p + half)
        tokblk[p] = jnp.concatenate(
            [xv[:, q0 : q0 + SLOT], xv[:, q1 : q1 + SLOT], jnp.zeros((8, PAIR - BLOCK), f32)], axis=1)
    c_ids()
    c_ew()
    c_mgain()
    idp[...] = jnp.full_like(idp, -1)
    ewp[...] = jnp.zeros_like(ewp)
    idp[0:seqs, 0 : ids.shape[1]] = ids_v[...]
    ewp[0:seqs, 0 : ids.shape[1]] = ew_v[...]
    idv, ewv = idp[...], ewp[...]
    rid = wrap((idv >> 2) - z, n_z) * NX + wrap((idv & 3) - x, NX)
    rid = jnp.where(idv < 0, -1, rid)
    slot_l, rank_l = lane >> 1, lane & 1
    hit, wsum = jnp.zeros((8, 128), f32), jnp.zeros((8, 128), f32)
    for k in range(ids.shape[1]):
        m = rid[:, k : k + 1] == slot_l
        hit = jnp.where(m, 1.0, hit)
        wsum = jnp.where(m, ewv[:, k : k + 1], wsum)
    rank = jnp.zeros((8, 128), f32)
    for s in range(seqs):
        rank += jnp.where(row8 > s, hit[s : s + 1, :], 0.0)
    place = jnp.where(rank == rank_l.astype(f32), hit, 0.0)
    comb = place * wsum
    comb_hi = comb.astype(bf16)
    comb_lo = (comb - comb_hi.astype(f32)).astype(bf16)
    comb2 = jnp.concatenate([comb_hi.astype(f32), comb_lo.astype(f32)], axis=0).astype(bf16)
    place_t = jnp.concatenate([place, jnp.zeros((120, 128), f32)], axis=0).T.astype(bf16)
    c_dn()
    flipped = jnp.concatenate(
        [dcat[:, pl.ds(128 * i, 128)].astype(f32).T for i in range(width // 128)], axis=0)
    for t in range(n_tp):
        dnt[t] = flipped[SLOT * t : SLOT * t + FOLD].astype(bf16)
        drem[t] = jnp.concatenate(
            [jnp.zeros((128, FOLD - 16), f32), dcat[:, SLOT * t + FOLD : SLOT * (t + 1)].astype(f32)],
            axis=1).astype(bf16)
    mg = mgain_v[...].astype(f32).reshape(1, width)
    c_wt()
    for i in range(4):
        rows = pl.ds(64 * i, 64)
        w = wt[rows, :].astype(f32) * mg
        tails = []
        for p in range(half):
            q0, q1 = SLOT * p, SLOT * (p + half)
            wp[p, rows, :] = jnp.concatenate(
                [w[:, q0 : q0 + SLOT], w[:, q1 : q1 + HEADK - SLOT]], axis=1).astype(bf16)
            tails.append(w[:, q1 + HEADK - SLOT : q1 + SLOT])
        wp[half, rows, :] = jnp.concatenate(tails, axis=1).astype(bf16)
    own_part = send1[pair].astype(f32)
    own_tok = tokblk[pair]
    whole(recv1, rsem.at[0])
    attn = own_part + jnp.sum(recv1[...].astype(f32), axis=0)
    lane2 = lax.broadcasted_iota(i32, (8, PAIR), 1)
    mixed = jnp.where(lane2 < BLOCK, own_tok + attn, 0.0).astype(bf16)
    mixed_f = mixed.astype(f32)

    mixed_p = jnp.concatenate([mixed_f, jnp.zeros((120, PAIR), f32)], axis=0).astype(bf16)
    rows = mm(place_t, mixed_p)[0 : 2 * n_ep].astype(bf16)
    send2[...] = rows.reshape(n_ep, 2, PAIR)

    for slot in slots:
        pltpu.make_async_remote_copy(
            src_ref=send2.at[slot], dst_ref=recv2.at[slot], send_sem=ssem.at[1], recv_sem=rsem.at[1],
            device_id={"ep": ep_at(slot)}, device_id_type=MESH).start()
    recv2[0] = send2[0]
    w_copy = pltpu.make_async_remote_copy(
        src_ref=wp.at[:, pl.ds(0, 256)], dst_ref=wp.at[:, pl.ds(256, 256)], send_sem=wsem.at[0],
        recv_sem=wsem.at[1], device_id=sibling, device_id_type=MESH)
    w_copy.start()
    for v in range(n_y):
        pltpu.make_async_remote_copy(
            src_ref=dnt.at[v * 2 + 1 - c], dst_ref=dsib.at[v], send_sem=wsem.at[2], recv_sem=wsem.at[3],
            device_id=sibling, device_id_type=MESH).start()
        pltpu.make_async_remote_copy(
            src_ref=drem.at[v * 2 + 1 - c], dst_ref=dsibr.at[v], send_sem=wsem.at[4], recv_sem=wsem.at[5],
            device_id=sibling, device_id_type=MESH).start()
    pltpu.make_async_copy(recv2.at[pl.ds(1, n_ep - 1)], recv2.at[pl.ds(1, n_ep - 1)], rsem.at[1]).wait()
    got = recv2[...].reshape(2 * n_ep, PAIR).astype(f32)
    rows_t = jnp.concatenate([got, mixed_f, jnp.zeros((120 - 2 * n_ep, PAIR), f32)], axis=0).T
    xt[pair] = rows_t[0:BLOCK].astype(bf16)

    upper = y // (n_y // 2)

    moves = (2, n_y - 2, 1, n_y - 1)
    hands = moves + (0,)

    def pair_at(dy, core):
        return lax.rem(y + dy, n_y // 2) * 2 + core

    def gather_copy(dy):
        if dy in (1, n_y - 1):
            part = xt.at[pair]
        else:
            part = xt.at[pair, pl.ds(pl.multiple_of(upper * SLOT, 16), SLOT)]
        return pltpu.make_async_remote_copy(
            src_ref=part, dst_ref=part, send_sem=ssem.at[4], recv_sem=r3.at[moves.index(dy)],
            device_id={"tp": lax.rem(me_tp + 2 * dy, n_tp)}, device_id_type=MESH)

    def hand_copy(dy):
        from_y = lax.rem(y + n_y - dy, n_y)
        if dy in (0, 1, n_y - 1):
            part = xt.at[pair_at(n_y - dy, c)]
        else:
            part = xt.at[pair_at(n_y - dy, c), pl.ds(pl.multiple_of(from_y // (n_y // 2) * SLOT, 16), SLOT)]
        return pltpu.make_async_remote_copy(
            src_ref=part, dst_ref=part, send_sem=ssem.at[5], recv_sem=f3r.at[hands.index(dy)],
            device_id=sibling, device_id_type=MESH)

    def products(dy, core):
        p = pair_at(n_y - dy, core)
        block = xt[p]
        wide = block.astype(f32)
        return mm(wp[p], block[0:HEADK]), jnp.sum(wide * wide, axis=0, keepdims=True)

    for dy in moves:
        gather_copy(dy).start()
    hand_copy(0).start()
    pltpu.make_async_copy(wp.at[:, pl.ds(256, 256)], wp.at[:, pl.ds(256, 256)], wsem.at[1]).wait()
    hid, squares = products(0, c)
    for dy in (1, n_y - 1):
        gather_copy(dy).wait_recv()
        hand_copy(dy).start()
    for dy in (1, n_y - 1):
        more = products(dy, c)
        hid, squares = hid + more[0], squares + more[1]
    hand_copy(0).wait_recv()
    more = products(0, 1 - c)
    hid, squares = hid + more[0], squares + more[1]
    for dy in (2, n_y - 2):
        gather_copy(dy).wait_recv()
        hand_copy(dy).start()
    more = products(2, c)
    hid, squares = hid + more[0], squares + more[1]
    for dy in (1, n_y - 1):
        hand_copy(dy).wait_recv()
        more = products(dy, 1 - c)
        hid, squares = hid + more[0], squares + more[1]
    whole(dsib, wsem.at[3])
    whole(dsibr, wsem.at[5])
    for dy in (2, n_y - 2):
        hand_copy(dy).wait_recv()
    more = products(2, 1 - c)
    hid, squares = hid + more[0], squares + more[1]
    tails = jnp.concatenate([xt[p, pl.ds(HEADK, TAILK), :] for p in range(half)], axis=0)
    hid = (hid + mm(wp[half], tails)) * lax.rsqrt(squares * (1.0 / width) + EPS)
    routed_l = lax.broadcasted_iota(i32, (64, 128), 1) < 2 * n_ep
    parts = []
    for o in (0, 256):
        ge, ue, gs, us = (hid[o + 64 * i : o + 64 * (i + 1)] for i in range(4))
        parts.append(jnp.where(routed_l, ge / (1.0 + jnp.exp(-ge)) * ue, 0.0))
        parts.append(jnp.where(routed_l, 0.0, gs / (1.0 + jnp.exp(-gs)) * us))
    hcat = jnp.concatenate(parts, axis=0)
    hrow = hcat.T[0:FOLD].astype(bf16)
    hcat = hcat.astype(bf16)

    far = (3, n_y - 3, 2, n_y - 2, 1, n_y - 1)
    far_at = {dy: i for i, dy in enumerate(far)}

    def sum_copy(dy):
        to = lax.rem(y + dy, n_y)
        v = to if dy < n_y // 2 else lax.rem(to + n_y - 1, n_y)
        return pltpu.make_async_remote_copy(
            src_ref=q5.at[v], dst_ref=recv5.at[far_at[dy]], send_sem=ssem.at[6], recv_sem=rsem.at[4],
            device_id={"tp": to * 2 + c}, device_id_type=MESH)

    def terms(v):
        t = v * 2 + c
        return mm(jnp.concatenate([dnt[t], dsib[v]], axis=1), hcat) + mm(
            hrow, jnp.concatenate([drem[t], dsibr[v]], axis=0))

    for dy in far:
        to = lax.rem(y + dy, n_y)
        v = to if dy < n_y // 2 else lax.rem(to + n_y - 1, n_y)
        q5[v] = terms(v).astype(bf16)
        sum_copy(dy).start()
    totals = [terms(y), terms(lax.rem(y + n_y - 1, n_y))]
    whole(recv5, rsem.at[4])
    for dy in far:
        side = 0 if dy < n_y // 2 else 1
        totals[side] += recv5[far_at[dy]].astype(f32)
    backs = []
    for a in totals:
        a = jnp.concatenate([a, jnp.zeros((128 - FOLD, 128), f32)], axis=0)
        backs.append(jnp.concatenate(
            [a.T[:, 0:FOLD], a[:, 128 - (SLOT - FOLD) : 128], jnp.zeros((128, LANES - SLOT), f32)], axis=1))
    shared = backs[0][2 * n_ep : 2 * n_ep + 8]
    share_s[...] = backs[1][2 * n_ep : 2 * n_ep + 8]
    for side in range(2):
        send6[side] = backs[side][0 : 2 * n_ep].astype(bf16).reshape(n_ep, 2, LANES)

    for slot in slots + [0]:
        for side in (1, 0) if slot else (1,):
            pltpu.make_async_remote_copy(
                src_ref=send6.at[side, slot], dst_ref=recv6.at[side, slot],
                send_sem=ssem.at[2 + side], recv_sem=rsem.at[2 + side],
                device_id={"ep": ep_back(slot), "tp": below if side else me_tp}, device_id_type=MESH).start()
    share_copy = pltpu.make_async_remote_copy(
        src_ref=share_s, dst_ref=share_r, send_sem=hsem.at[0], recv_sem=hsem.at[1],
        device_id={"tp": below}, device_id_type=MESH)
    share_copy.start()
    recv6[0, 0] = send6[0, 0]
    whole(recv1, ssem.at[0])
    pltpu.make_async_copy(recv2.at[pl.ds(1, n_ep - 1)], recv2.at[pl.ds(1, n_ep - 1)], ssem.at[1]).wait()
    w_copy.wait_send()
    whole(dsib, wsem.at[2])
    whole(dsibr, wsem.at[4])
    whole(xt.at[pl.ds(0, 3)], ssem.at[4])
    whole(xt.at[pl.ds(0, 4)], ssem.at[5])
    whole(recv5, ssem.at[6])
    share_copy.wait_recv()
    whole(recv6.at[0, pl.ds(1, n_ep - 1)], rsem.at[2])
    whole(recv6.at[1], rsem.at[3])
    shared = shared + share_r[...]
    two = sum(mm(comb2[:, 0 : 2 * n_ep], recv6[side].reshape(2 * n_ep, LANES)) for side in range(2))
    mine = jnp.where(y >= n_y // 2, mixed_f[:, SLOT : BLOCK], mixed_f[:, 0:SLOT])
    res = mine + ((two[0:8] + two[8:16]) + shared)[:, 0:SLOT]
    out[...] = res[0:seqs].astype(bf16)
    whole(recv6.at[0, pl.ds(1, n_ep - 1)], ssem.at[2])
    whole(recv6.at[1], ssem.at[3])
    share_copy.wait_send()


def solution(mesh):
    n_ep, n_tp = mesh.shape["ep"], mesh.shape["tp"]
    n_y = half = n_tp // 2

    def step(tokens, attn_gain, wq, wk, wv, ow, lambdas, head_gain, ck, cv, lengths, moe_gain,
             gw, uw, dw, sg, su, sd, ids, ew):
        seqs, width = tokens.shape
        cache = ck.shape[1]
        pairs = (seqs + 1) // 2
        V, DMA = pltpu.VMEM, pltpu.SemaphoreType.DMA
        scratch = [
            V((seqs, width), bf16), V((width, 384), bf16), V((pairs, cache, 256), bf16), V((pairs, cache, 256), bf16),
            V((half, PAIR, 128), bf16), V((256, width), bf16), V((128, width), bf16),
            V((1, 1), f32), pltpu.SMEM((seqs,), i32), V((width,), bf16), V((128,), bf16), V((width,), bf16),
            V(ids.shape, i32), V(ew.shape, f32),
            V((8, width), f32), V((half, 8, PAIR), f32), V((8, 128), i32), V((8, 128), f32),
            V((n_tp, FOLD, 128), bf16), V((n_tp, 128, 128), bf16),
            V((n_y, FOLD, 128), bf16), V((n_y, 128, 128), bf16), V((half + 1, 512, HEADK), bf16),
            V((half, 8, PAIR), bf16), V((n_tp - 1, 8, PAIR), bf16),
            V((n_ep, 2, PAIR), bf16), V((n_ep, 2, PAIR), bf16),
            V((half, BLOCK, 128), bf16), V((n_y, FOLD, 128), bf16), V((n_y - 2, FOLD, 128), bf16),
            V((2, n_ep, 2, LANES), bf16), V((2, n_ep, 2, LANES), bf16), V((8, LANES), f32), V((8, LANES), f32),
            DMA((24,)), DMA((7,)), DMA((5,)), DMA((4,)), DMA((5,)), DMA((6,)), DMA((2,)),
        ]
        return pl.pallas_call(
            functools.partial(kernel, n_ep, n_tp),
            out_shape=pltpu.VMEM((seqs, width // n_tp), bf16),
            in_specs=[pl.BlockSpec(memory_space=pl.ANY)] * 20,
            out_specs=pl.BlockSpec(memory_space=pltpu.VMEM),
            scratch_shapes=scratch,
            compiler_params=pltpu.CompilerParams(collective_id=0, has_side_effects=True),
            name="decode_step",
        )(tokens, attn_gain, wq, wk, wv, ow, lambdas.reshape(1, 1), head_gain,
          ck.reshape(seqs, cache, 128), cv.reshape(seqs, cache, 128), lengths, moe_gain,
          gw[0].T, uw[0].T, dw[0], sg.T, su.T, sd, ids, ew)

    in_specs = (
        P("ep", None), P(), P(None, "tp"), P(None, "tp"), P(None, "tp"), P(None, "tp"), P("tp"), P(),
        P("ep", None, "tp", None), P("ep", None, "tp", None), P("ep"), P(),
        P("ep", None, "tp"), P("ep", None, "tp"), P("ep", "tp", None),
        P(None, "tp"), P(None, "tp"), P("tp", None), P("ep", None), P("ep", None),
    )
    return jax.shard_map(step, mesh=mesh, in_specs=in_specs, out_specs=P("ep", "tp"), check_vma=False)
```

```python
import functools

import jax
import jax.numpy as jnp
from jax import lax
from jax.experimental import pallas as pl
from jax.experimental.pallas import tpu as pltpu
from jax.sharding import PartitionSpec as P

EPS = 1e-06
NX = 4
MESH = pl.DeviceIdType.MESH
NT = (((1,), (1,)), ((), ()))
bf16, f32, i32 = jnp.bfloat16, jnp.float32, jnp.int32
SLOT = 144
LANES = 256
BLOCK = 2 * SLOT
PAIR = 384
FOLD = 120
HEADK = 256
TAILK = BLOCK - HEADK


def wrap(v, n):
    return jnp.where(v < 0, v + n, v)


def mm(a, b):
    return jnp.dot(a, b, preferred_element_type=f32)


def mm_nt(a, b):
    return lax.dot_general(a, b, NT, preferred_element_type=f32)


def kernel(
    n_ep, n_tp,
    tok, again, wq, wk, wv, ow, lam, hgain, ck, cv, lens, mgain, gwt, uwt, dw, sgt, sut, sd, ids, ew,
    out,
    tok_v, wqkv, k_v, v_v, ow_v, wt, dcat, lam_v, lens_s, again_v, hgain_v, mgain_v, ids_v, ew_v,
    x_s, tokblk, idp, ewp, dnt, drem, dsib, dsibr, wp,
    send1, recv1, send2, recv2, xt, q5, recv5, send6, recv6, share_s, share_r,
    lsem, ssem, rsem, r3, f3r, wsem, hsem, here,
):
    n_z, n_y = n_ep // NX, n_tp // 2
    seqs, width = tok.shape
    cache = ck.shape[1]
    me_ep, me_tp = lax.axis_index("ep"), lax.axis_index("tp")
    z, x = me_ep // NX, lax.rem(me_ep, NX)
    y, c = me_tp // 2, lax.rem(me_tp, 2)

    half = n_tp // 2
    pair = lax.rem(me_tp, half)
    other = lax.rem(me_tp + half, n_tp)
    sibling = {"tp": y * 2 + 1 - c}
    below = lax.rem(me_tp + n_tp - 2, n_tp)
    z_at = [wrap(z + d - n_z, n_z) * NX for d in range(n_z)]
    x_at = [wrap(x + d - NX, NX) for d in range(NX)]

    def hops(slot):
        dz, dx = slot // NX, slot % NX
        return min(dz, n_z - dz) + min(dx, NX - dx)

    slots = sorted(range(1, n_ep), key=lambda s: -hops(s))

    def ep_at(slot):
        return z_at[slot // NX] + x_at[slot % NX]

    def ep_back(slot):
        return z_at[-(slot // NX) % n_z] + x_at[-(slot % NX) % NX]

    bar = pltpu.get_barrier_semaphore()
    groups = []

    def load(pairs, region=None):
        sem = lsem.at[len(groups)]
        for src, dst in pairs:
            pltpu.make_async_copy(src, dst, sem).start()
        groups.append(region)
        region = pairs[0][1] if region is None else region
        return lambda: whole(region, sem)

    def whole(ref, sem):
        pltpu.make_async_copy(ref, ref, sem).wait()

    def cached(src, dst):
        return [
            load([(src.at[s], dst.at[p, :, pl.ds(128 * (s % 2), 128)]) for s in range(2 * p, min(2 * p + 2, seqs))],
                 dst.at[p, :, pl.ds(0, 128 * min(2, seqs - 2 * p))])
            for p in range((seqs + 1) // 2)]

    c_tok, c_gain = load([(tok, tok_v)]), load([(again, again_v)])
    step = width // 3
    c_qkv = [
        load([(w.at[pl.ds(step * j, step)], wqkv.at[pl.ds(step * j, step), pl.ds(128 * i, 128)])
              for i, w in enumerate((wq, wk, wv))], wqkv.at[pl.ds(step * j, step)])
        for j in range(3)]
    for r in range(1, n_tp):
        pl.semaphore_signal(bar, inc=1, device_id={"tp": lax.rem(me_tp + r, n_tp)}, device_id_type=MESH)
    c_k = cached(ck, k_v)
    c_len, c_lam, c_hgain = load([(lens, lens_s)]), load([(lam, lam_v)]), load([(hgain, hgain_v)])
    c_v = cached(cv, v_v)
    c_ow = load(
        [(ow.at[pl.ds(SLOT * t, SLOT)], ow_v.at[t % half, pl.ds(SLOT * (t // half), SLOT)]) for t in range(n_tp)],
        ow_v.at[:, pl.ds(0, BLOCK)])
    c_ids, c_ew, c_mgain = load([(ids, ids_v)]), load([(ew, ew_v)]), load([(mgain, mgain_v)])
    c_dn = load([(w, dcat.at[pl.ds(64 * i, 64)]) for i, w in enumerate((dw, sd))], dcat)
    c_wt = load([(w, wt.at[pl.ds(64 * i, 64)]) for i, w in enumerate((gwt, uwt, sgt, sut))], wt)

    for slot in slots:
        greeted = ep_at(slot)

        @pl.when(greeted > me_ep)
        def greet():
            pl.semaphore_signal(bar, inc=1, device_id={"ep": greeted}, device_id_type=MESH)

    x_s[...] = jnp.zeros_like(x_s)
    if seqs % 2:
        k_v[seqs // 2, :, pl.ds(128, 128)] = jnp.zeros((cache, 128), bf16)
        v_v[seqs // 2, :, pl.ds(128, 128)] = jnp.zeros((cache, 128), bf16)
    c_tok()
    c_gain()
    x_s[0:seqs, :] = tok_v[...].astype(f32)
    xv = x_s[...]
    gain = again_v[...].astype(f32).reshape(1, width)
    normed = (xv * lax.rsqrt(jnp.mean(xv * xv, axis=-1, keepdims=True) + EPS) * gain).astype(bf16)
    qkv = jnp.zeros((8, 384), f32)
    for j in range(3):
        c_qkv[j]()
        qkv += mm(normed[:, step * j : step * (j + 1)], wqkv[pl.ds(step * j, step), :])
    qkv = qkv.astype(bf16).astype(f32)
    q, kn, vn = qkv[:, 0:128], qkv[:, 128:256], qkv[:, 256:384]
    lane = lax.broadcasted_iota(i32, (8, 128), 1)
    first = lane < 64
    qk = q * kn
    scale = 0.125
    own = jnp.concatenate(
        [jnp.sum(jnp.where(first, qk, 0.0), axis=-1, keepdims=True),
         jnp.sum(jnp.where(first, 0.0, qk), axis=-1, keepdims=True)], axis=0) * scale
    q2 = jnp.concatenate([jnp.where(first, q, 0.0), jnp.where(first, 0.0, q)], axis=0)
    row16 = lax.broadcasted_iota(i32, (16, 128), 0)
    row16 = jnp.where(row16 >= 8, row16 - 8, row16)
    scores = jnp.zeros((16, cache), f32)
    c_len()
    c_lam()
    c_hgain()
    for p in range((seqs + 1) // 2):
        c_k[p]()
        qa = jnp.where(row16 == 2 * p, q2, 0.0)
        qb = jnp.where(row16 == 2 * p + 1, q2, 0.0)
        scores += mm_nt(jnp.concatenate([qa, qb], axis=1).astype(bf16), k_v[p])
    scores = scores * scale
    rcol = lax.broadcasted_iota(i32, (16, 1), 0)
    rcol = jnp.where(rcol >= 8, rcol - 8, rcol)
    lcol = jnp.zeros((16, 1), i32)
    for s in range(seqs):
        lcol = jnp.where(rcol == s, lens_s[s], lcol)
    live = lax.broadcasted_iota(i32, (16, cache), 1) < lcol
    peak = jnp.maximum(jnp.max(jnp.where(live, scores, -jnp.inf), axis=-1, keepdims=True), own)
    terms = jnp.where(live, jnp.exp(scores - peak), 0.0)
    own_term = jnp.exp(own - peak)
    inv = 1.0 / (jnp.sum(terms, axis=-1, keepdims=True) + own_term)
    probs, own_prob = terms * inv, own_term * inv
    lm = lam_v[...]
    mix = (probs[0:8] - lm * probs[8:16]).astype(bf16).astype(f32)
    own_mix = (own_prob[0:8] - lm * own_prob[8:16]).astype(bf16).astype(f32)
    rowc = lax.broadcasted_iota(i32, (8, cache), 0)
    both = jnp.zeros((8, 256), f32)
    for p in range((seqs + 1) // 2):
        c_v[p]()
        both += mm(jnp.where(rowc // 2 == p, mix, 0.0).astype(bf16), v_v[p])
    row8 = lax.broadcasted_iota(i32, (8, 128), 0)
    head = jnp.where(row8 % 2 == 0, both[:, 0:128], both[:, 128:256]) + own_mix * vn
    hg = hgain_v[...].astype(f32).reshape(1, 128)
    head_n = (head * lax.rsqrt(jnp.mean(head * head, axis=-1, keepdims=True) + EPS) * hg).astype(bf16)
    c_ow()
    tail = ow_v[:, pl.ds(HEADK, TAILK), :]
    for k in range(1, 8):
        ow_v[:, pl.ds(HEADK + TAILK * k, TAILK), :] = tail
    part = mm_nt(head_n, ow_v[...].reshape(half * 2 * HEADK, 128))
    row_h = lax.broadcasted_iota(i32, (8, HEADK), 0)
    in_tail = lax.broadcasted_iota(i32, (8, HEADK), 1) // TAILK == row_h
    for p in range(half):
        o = 2 * HEADK * p
        tails = jnp.sum(jnp.where(in_tail, part[:, o + HEADK : o + 2 * HEADK], 0.0), axis=0, keepdims=True)
        send1[p] = jnp.where(row_h == 7, tails, part[:, o : o + HEADK]).astype(bf16)

    pl.semaphore_wait(bar, n_tp - 1 + me_ep)
    for r in sorted(range(1, n_tp), key=lambda r: -min(r, n_tp - r)):
        to = lax.rem(me_tp + r, n_tp)
        pltpu.make_async_remote_copy(
            src_ref=send1.at[lax.rem(to, half)], dst_ref=recv1.at[r - 1], send_sem=ssem.at[0], recv_sem=rsem.at[0],
            device_id={"tp": to}, device_id_type=MESH).start()

    for slot in slots:
        answered = ep_at(slot)

        @pl.when(answered < me_ep)
        def answer():
            pl.semaphore_signal(here, inc=1, device_id={"ep": answered}, device_id_type=MESH)

    for p in range(half):
        q0, q1 = SLOT * p, SLOT * (p + half)
        tokblk[p] = jnp.concatenate(
            [xv[:, q0 : q0 + SLOT], xv[:, q1 : q1 + SLOT], jnp.zeros((8, PAIR - BLOCK), f32)], axis=1)
    c_ids()
    c_ew()
    c_mgain()
    idp[...] = jnp.full_like(idp, -1)
    ewp[...] = jnp.zeros_like(ewp)
    idp[0:seqs, 0 : ids.shape[1]] = ids_v[...]
    ewp[0:seqs, 0 : ids.shape[1]] = ew_v[...]
    idv, ewv = idp[...], ewp[...]
    rid = wrap((idv >> 2) - z, n_z) * NX + wrap((idv & 3) - x, NX)
    rid = jnp.where(idv < 0, -1, rid)
    slot_l, rank_l = lane >> 1, lane & 1
    hit, wsum = jnp.zeros((8, 128), f32), jnp.zeros((8, 128), f32)
    for k in range(ids.shape[1]):
        m = rid[:, k : k + 1] == slot_l
        hit = jnp.where(m, 1.0, hit)
        wsum = jnp.where(m, ewv[:, k : k + 1], wsum)
    rank = jnp.zeros((8, 128), f32)
    for s in range(seqs):
        rank += jnp.where(row8 > s, hit[s : s + 1, :], 0.0)
    place = jnp.where(rank == rank_l.astype(f32), hit, 0.0)
    comb = place * wsum
    comb_hi = comb.astype(bf16)
    comb_lo = (comb - comb_hi.astype(f32)).astype(bf16)
    comb2 = jnp.concatenate([comb_hi.astype(f32), comb_lo.astype(f32)], axis=0).astype(bf16)
    place_t = jnp.concatenate([place, jnp.zeros((120, 128), f32)], axis=0).T.astype(bf16)
    c_dn()
    flipped = jnp.concatenate(
        [dcat[:, pl.ds(128 * i, 128)].astype(f32).T for i in range(width // 128)], axis=0)
    for t in range(n_tp):
        dnt[t] = flipped[SLOT * t : SLOT * t + FOLD].astype(bf16)
        drem[t] = jnp.concatenate(
            [jnp.zeros((128, FOLD - 16), f32), dcat[:, SLOT * t + FOLD : SLOT * (t + 1)].astype(f32)],
            axis=1).astype(bf16)
    mg = mgain_v[...].astype(f32).reshape(1, width)
    c_wt()
    for i in range(4):
        rows = pl.ds(64 * i, 64)
        w = wt[rows, :].astype(f32) * mg
        tails = []
        for p in range(half):
            q0, q1 = SLOT * p, SLOT * (p + half)
            wp[p, rows, :] = jnp.concatenate(
                [w[:, q0 : q0 + SLOT], w[:, q1 : q1 + HEADK - SLOT]], axis=1).astype(bf16)
            tails.append(w[:, q1 + HEADK - SLOT : q1 + SLOT])
        wp[half, rows, :] = jnp.concatenate(tails, axis=1).astype(bf16)
    own_part = send1[pair].astype(f32)
    own_tok = tokblk[pair]
    whole(recv1, rsem.at[0])
    sums = own_part + jnp.sum(recv1[...].astype(f32), axis=0)
    tails = jnp.where(in_tail, sums[7:8, :], 0.0)
    tails = tails[:, 0:128] + tails[:, 128:256]
    tails = tails + pltpu.roll(tails, 64, 1)
    tails = tails + pltpu.roll(tails, 32, 1)
    attn = jnp.concatenate([jnp.where(row_h == 7, 0.0, sums), tails], axis=1)
    lane2 = lax.broadcasted_iota(i32, (8, PAIR), 1)
    mixed = jnp.where(lane2 < BLOCK, own_tok + attn, 0.0).astype(bf16)
    mixed_f = mixed.astype(f32)

    mixed_p = jnp.concatenate([mixed_f, jnp.zeros((120, PAIR), f32)], axis=0).astype(bf16)
    rows = mm(place_t, mixed_p)[0 : 2 * n_ep].astype(bf16)
    send2[...] = rows.reshape(n_ep, 2, PAIR)

    @pl.when(me_ep < n_ep - 1)
    def answers():
        pl.semaphore_wait(here, n_ep - 1 - me_ep)

    for slot in slots:
        pltpu.make_async_remote_copy(
            src_ref=send2.at[slot], dst_ref=recv2.at[slot], send_sem=ssem.at[1], recv_sem=rsem.at[1],
            device_id={"ep": ep_at(slot)}, device_id_type=MESH).start()
    recv2[0] = send2[0]
    w_copy = pltpu.make_async_remote_copy(
        src_ref=wp.at[:, pl.ds(0, 256)], dst_ref=wp.at[:, pl.ds(256, 256)], send_sem=wsem.at[0],
        recv_sem=wsem.at[1], device_id=sibling, device_id_type=MESH)
    w_copy.start()
    for v in range(n_y):
        pltpu.make_async_remote_copy(
            src_ref=dnt.at[v * 2 + 1 - c], dst_ref=dsib.at[v], send_sem=wsem.at[2], recv_sem=wsem.at[3],
            device_id=sibling, device_id_type=MESH).start()
        pltpu.make_async_remote_copy(
            src_ref=drem.at[v * 2 + 1 - c], dst_ref=dsibr.at[v], send_sem=wsem.at[4], recv_sem=wsem.at[5],
            device_id=sibling, device_id_type=MESH).start()
    pltpu.make_async_copy(recv2.at[pl.ds(1, n_ep - 1)], recv2.at[pl.ds(1, n_ep - 1)], rsem.at[1]).wait()
    got = recv2[...].reshape(2 * n_ep, PAIR).astype(f32)
    rows_t = jnp.concatenate([got, mixed_f, jnp.zeros((120 - 2 * n_ep, PAIR), f32)], axis=0).T
    xt[pair] = rows_t[0:BLOCK].astype(bf16)

    upper = y // (n_y // 2)

    moves = (2, n_y - 2, 1, n_y - 1)
    hands = moves + (0,)

    def pair_at(dy, core):
        return lax.rem(y + dy, n_y // 2) * 2 + core

    def gather_copy(dy):
        if dy in (1, n_y - 1):
            part = xt.at[pair]
        else:
            part = xt.at[pair, pl.ds(pl.multiple_of(upper * SLOT, 16), SLOT)]
        return pltpu.make_async_remote_copy(
            src_ref=part, dst_ref=part, send_sem=ssem.at[4], recv_sem=r3.at[moves.index(dy)],
            device_id={"tp": lax.rem(me_tp + 2 * dy, n_tp)}, device_id_type=MESH)

    def hand_copy(dy):
        from_y = lax.rem(y + n_y - dy, n_y)
        if dy in (0, 1, n_y - 1):
            part = xt.at[pair_at(n_y - dy, c)]
        else:
            part = xt.at[pair_at(n_y - dy, c), pl.ds(pl.multiple_of(from_y // (n_y // 2) * SLOT, 16), SLOT)]
        return pltpu.make_async_remote_copy(
            src_ref=part, dst_ref=part, send_sem=ssem.at[5], recv_sem=f3r.at[hands.index(dy)],
            device_id=sibling, device_id_type=MESH)

    def products(dy, core):
        p = pair_at(n_y - dy, core)
        block = xt[p]
        wide = block.astype(f32)
        return mm(wp[p], block[0:HEADK]), jnp.sum(wide * wide, axis=0, keepdims=True)

    for dy in moves:
        gather_copy(dy).start()
    hand_copy(0).start()
    pltpu.make_async_copy(wp.at[:, pl.ds(256, 256)], wp.at[:, pl.ds(256, 256)], wsem.at[1]).wait()
    hid, squares = products(0, c)
    for dy in (1, n_y - 1):
        gather_copy(dy).wait_recv()
        hand_copy(dy).start()
    for dy in (1, n_y - 1):
        more = products(dy, c)
        hid, squares = hid + more[0], squares + more[1]
    hand_copy(0).wait_recv()
    more = products(0, 1 - c)
    hid, squares = hid + more[0], squares + more[1]
    for dy in (2, n_y - 2):
        gather_copy(dy).wait_recv()
        hand_copy(dy).start()
    more = products(2, c)
    hid, squares = hid + more[0], squares + more[1]
    for dy in (1, n_y - 1):
        hand_copy(dy).wait_recv()
        more = products(dy, 1 - c)
        hid, squares = hid + more[0], squares + more[1]
    whole(dsib, wsem.at[3])
    whole(dsibr, wsem.at[5])
    for dy in (2, n_y - 2):
        hand_copy(dy).wait_recv()
    more = products(2, 1 - c)
    hid, squares = hid + more[0], squares + more[1]
    tails = jnp.concatenate([xt[p, pl.ds(HEADK, TAILK), :] for p in range(half)], axis=0)
    hid = (hid + mm(wp[half], tails)) * lax.rsqrt(squares * (1.0 / width) + EPS)
    routed_l = lax.broadcasted_iota(i32, (64, 128), 1) < 2 * n_ep
    parts = []
    for o in (0, 256):
        ge, ue, gs, us = (hid[o + 64 * i : o + 64 * (i + 1)] for i in range(4))
        parts.append(jnp.where(routed_l, ge / (1.0 + jnp.exp(-ge)) * ue, 0.0))
        parts.append(jnp.where(routed_l, 0.0, gs / (1.0 + jnp.exp(-gs)) * us))
    hcat = jnp.concatenate(parts, axis=0)
    hrow = hcat.T[0:FOLD].astype(bf16)
    hcat = hcat.astype(bf16)

    far = (3, n_y - 3, 2, n_y - 2, 1, n_y - 1)
    far_at = {dy: i for i, dy in enumerate(far)}

    def sum_copy(dy):
        to = lax.rem(y + dy, n_y)
        v = to if dy < n_y // 2 else lax.rem(to + n_y - 1, n_y)
        return pltpu.make_async_remote_copy(
            src_ref=q5.at[v], dst_ref=recv5.at[far_at[dy]], send_sem=ssem.at[6], recv_sem=rsem.at[4],
            device_id={"tp": to * 2 + c}, device_id_type=MESH)

    def terms(v):
        t = v * 2 + c
        return mm(jnp.concatenate([dnt[t], dsib[v]], axis=1), hcat) + mm(
            hrow, jnp.concatenate([drem[t], dsibr[v]], axis=0))

    for dy in far:
        to = lax.rem(y + dy, n_y)
        v = to if dy < n_y // 2 else lax.rem(to + n_y - 1, n_y)
        q5[v] = terms(v).astype(bf16)
        sum_copy(dy).start()
    totals = [terms(y), terms(lax.rem(y + n_y - 1, n_y))]
    whole(recv5, rsem.at[4])
    for dy in far:
        side = 0 if dy < n_y // 2 else 1
        totals[side] += recv5[far_at[dy]].astype(f32)
    backs = []
    for a in totals:
        a = jnp.concatenate([a, jnp.zeros((128 - FOLD, 128), f32)], axis=0)
        backs.append(jnp.concatenate(
            [a.T[:, 0:FOLD], a[:, 128 - (SLOT - FOLD) : 128], jnp.zeros((128, LANES - SLOT), f32)], axis=1))
    shared = backs[0][2 * n_ep : 2 * n_ep + 8]
    share_s[...] = backs[1][2 * n_ep : 2 * n_ep + 8]
    for side in range(2):
        send6[side] = backs[side][0 : 2 * n_ep].astype(bf16).reshape(n_ep, 2, LANES)

    for slot in slots + [0]:
        for side in (1, 0) if slot else (1,):
            pltpu.make_async_remote_copy(
                src_ref=send6.at[side, slot], dst_ref=recv6.at[side, slot],
                send_sem=ssem.at[2 + side], recv_sem=rsem.at[2 + side],
                device_id={"ep": ep_back(slot), "tp": below if side else me_tp}, device_id_type=MESH).start()
    share_copy = pltpu.make_async_remote_copy(
        src_ref=share_s, dst_ref=share_r, send_sem=hsem.at[0], recv_sem=hsem.at[1],
        device_id={"tp": below}, device_id_type=MESH)
    share_copy.start()
    recv6[0, 0] = send6[0, 0]
    whole(recv1, ssem.at[0])
    pltpu.make_async_copy(recv2.at[pl.ds(1, n_ep - 1)], recv2.at[pl.ds(1, n_ep - 1)], ssem.at[1]).wait()
    w_copy.wait_send()
    whole(dsib, wsem.at[2])
    whole(dsibr, wsem.at[4])
    whole(xt.at[pl.ds(0, 3)], ssem.at[4])
    whole(xt.at[pl.ds(0, 4)], ssem.at[5])
    whole(recv5, ssem.at[6])
    share_copy.wait_recv()
    whole(recv6.at[0, pl.ds(1, n_ep - 1)], rsem.at[2])
    whole(recv6.at[1], rsem.at[3])
    shared = shared + share_r[...]
    two = sum(mm(comb2[:, 0 : 2 * n_ep], recv6[side].reshape(2 * n_ep, LANES)) for side in range(2))
    mine = jnp.where(y >= n_y // 2, mixed_f[:, SLOT : BLOCK], mixed_f[:, 0:SLOT])
    res = mine + ((two[0:8] + two[8:16]) + shared)[:, 0:SLOT]
    out[...] = res[0:seqs].astype(bf16)
    whole(recv6.at[0, pl.ds(1, n_ep - 1)], ssem.at[2])
    whole(recv6.at[1], ssem.at[3])
    share_copy.wait_send()


def solution(mesh):
    n_ep, n_tp = mesh.shape["ep"], mesh.shape["tp"]
    n_y = half = n_tp // 2

    def step(tokens, attn_gain, wq, wk, wv, ow, lambdas, head_gain, ck, cv, lengths, moe_gain,
             gw, uw, dw, sg, su, sd, ids, ew):
        seqs, width = tokens.shape
        cache = ck.shape[1]
        pairs = (seqs + 1) // 2
        V, DMA = pltpu.VMEM, pltpu.SemaphoreType.DMA
        scratch = [
            V((seqs, width), bf16), V((width, 384), bf16), V((pairs, cache, 256), bf16), V((pairs, cache, 256), bf16),
            V((half, 2 * HEADK, 128), bf16), V((256, width), bf16), V((128, width), bf16),
            V((1, 1), f32), pltpu.SMEM((seqs,), i32), V((width,), bf16), V((128,), bf16), V((width,), bf16),
            V(ids.shape, i32), V(ew.shape, f32),
            V((8, width), f32), V((half, 8, PAIR), f32), V((8, 128), i32), V((8, 128), f32),
            V((n_tp, FOLD, 128), bf16), V((n_tp, 128, 128), bf16),
            V((n_y, FOLD, 128), bf16), V((n_y, 128, 128), bf16), V((half + 1, 512, HEADK), bf16),
            V((half, 8, HEADK), bf16), V((n_tp - 1, 8, HEADK), bf16),
            V((n_ep, 2, PAIR), bf16), V((n_ep, 2, PAIR), bf16),
            V((half, BLOCK, 128), bf16), V((n_y, FOLD, 128), bf16), V((n_y - 2, FOLD, 128), bf16),
            V((2, n_ep, 2, LANES), bf16), V((2, n_ep, 2, LANES), bf16), V((8, LANES), f32), V((8, LANES), f32),
            DMA((24,)), DMA((7,)), DMA((5,)), DMA((4,)), DMA((5,)), DMA((6,)), DMA((2,)), pltpu.SemaphoreType.REGULAR,
        ]
        return pl.pallas_call(
            functools.partial(kernel, n_ep, n_tp),
            out_shape=pltpu.VMEM((seqs, width // n_tp), bf16),
            in_specs=[pl.BlockSpec(memory_space=pl.ANY)] * 20,
            out_specs=pl.BlockSpec(memory_space=pltpu.VMEM),
            scratch_shapes=scratch,
            compiler_params=pltpu.CompilerParams(collective_id=0, has_side_effects=True),
            name="decode_step",
        )(tokens, attn_gain, wq, wk, wv, ow, lambdas.reshape(1, 1), head_gain,
          ck.reshape(seqs, cache, 128), cv.reshape(seqs, cache, 128), lengths, moe_gain,
          gw[0].T, uw[0].T, dw[0], sg.T, su.T, sd, ids, ew)

    in_specs = (
        P("ep", None), P(), P(None, "tp"), P(None, "tp"), P(None, "tp"), P(None, "tp"), P("tp"), P(),
        P("ep", None, "tp", None), P("ep", None, "tp", None), P("ep"), P(),
        P("ep", None, "tp"), P("ep", None, "tp"), P("ep", "tp", None),
        P(None, "tp"), P(None, "tp"), P("tp", None), P("ep", None), P("ep", None),
    )
    return jax.shard_map(step, mesh=mesh, in_specs=in_specs, out_specs=P("ep", "tp"), check_vma=False)
```
